32 devices in a mesh: sp: 8 (over z, x), dp: 4 (over y, core).
Axes of the slice: x: 2, y: 2, z: 4, core: 2. Of those that a mesh axis runs over, the one named last changes fastest.
Arguments:
- layer_activity: bfloat16 [4, 1024, 2048], P('dp', 'sp'), may hold values from -6 to 6
- writer_matrix: bfloat16 [2048, 256], P('dp'), may hold values from -0.125 to 0.125
- reader_matrix: bfloat16 [2048, 256], P('dp'), may hold values from -0.125 to 0.125
- source_unfiltered: bfloat16 [4, 1024, 2048], P('dp', 'sp'), may hold values from -6 to 6
- switch_raw_signal: bfloat16 [4, 1024, 2048], P('dp', 'sp'), may hold values from -6 to 6
- saved_result: bfloat16 [4, 1024, 2048], P('dp', 'sp'), may hold values from -6 to 6
- final_adjoint: bfloat16 [4, 1024, 2048], P('dp', 'sp'), may hold values from -6 to 6
- delta_raw: bfloat16 [4, 1024, 32], P('dp', 'sp'), may hold values from -4 to 4
- extra_logdrop: float32 [4, 1024, 32], P('dp', None, 'sp'), may hold values from 0 to 2.1
- source_filter_coefs: float32 [5, 2048], P(None, 'sp'), may hold values from -2.5 to 2.5
- writer_filter_coefs: float32 [5, 256], replicated, may hold values from -2.5 to 2.5
- reader_filter_coefs: float32 [5, 256], replicated, may hold values from -2.5 to 2.5
- delta_offset: float32 [32], P('sp'), may hold values from -7.5 to -6
- fading_exponents: float32 [32], P('sp'), may hold values from -6 to 3.4
- direct_factor: float32 [32], P('sp'), may hold values from 0.1 to 1.9
- rescale_factor: float32 [2048], replicated, may hold values from 0.1 to 1.9
Outputs:
- d_hidden: bfloat16 [4, 1024, 2048], P('dp', 'sp')
- d_x_raw: bfloat16 [4, 1024, 2048], P('dp', 'sp')
- d_gate: bfloat16 [4, 1024, 2048], P('dp', 'sp')
- d_dt_raw: bfloat16 [4, 1024, 32], P('dp', 'sp')
- d_w_b: float32 [2048, 256], P('dp')
- d_w_c: float32 [2048, 256], P('dp')
The draws below stay inside these ranges and needn't reach their ends.
All inputs are finite; a program needn't handle non-finite values.
Results may differ from the reference program's by a relative error of at most 0.012.
Values may be sent and summed in bfloat16 or wider, within the bound.
No kernel may reach another device: no remote copies, remote signals or barrier semaphores. Data moves between devices by JAX's collectives and lax.ppermute only.
A program may use at most 128 MiB of HBM per device.

```python
import jax
import jax.numpy as jnp
from jax import lax

D = 2048
HEADS = 32
HEAD_DIM = 64
STATE = 128
GROUPS = 2
NORM_GROUPS = 8
CONV_K = 5
BLOCK = 128
TOK_DEV = 128
INNER = 2048
TOKEN_TOTAL = 1024
BATCH_TOTAL = 4


def draw_delta_raw(key, part):
    key_base, key_shift = jax.random.split(key)
    baseline = jnp.clip(0.7 * jax.random.normal(key_base, (BATCH_TOTAL, TOKEN_TOTAL, HEADS), jnp.float32), -2.8, 2.8)
    blocks = TOKEN_TOTAL // TOK_DEV
    shifts = jax.random.uniform(key_shift, (BATCH_TOTAL, blocks, 1, 1), jnp.float32, -1.0, 1.0)
    shifts = jnp.broadcast_to(shifts, (BATCH_TOTAL, blocks, TOK_DEV, 1)).reshape(BATCH_TOTAL, TOKEN_TOTAL, 1)
    return (baseline + shifts).astype(jnp.bfloat16)


def draw_extra_logdrop(key, part):
    key_where, key_size = jax.random.split(key)
    places = jax.random.randint(key_where, (3, BATCH_TOTAL, 1, HEADS), 0, TOKEN_TOTAL)
    amounts = jax.random.uniform(key_size, (3, BATCH_TOTAL, 1, HEADS), jnp.float32, 0.22, 0.69)
    positions = jnp.arange(TOKEN_TOTAL, dtype=jnp.int32)[None, None, :, None]
    return jnp.sum(jnp.where(positions == places, amounts, 0.0), axis=0)


def draw_fading_exponents(key, part):
    key_pick, key_fast, key_slow = jax.random.split(key, 3)
    fraction = 0.5
    picked = jax.random.uniform(key_pick, (HEADS,), jnp.float32) < fraction
    fast_rate = jax.random.uniform(key_fast, (HEADS,), jnp.float32, 2.3, 3.0)
    slow_rate = jnp.log(jax.random.uniform(key_slow, (HEADS,), jnp.float32, 0.2, 0.8) / (TOKEN_TOTAL * 0.0018))
    return jnp.where(picked, fast_rate, slow_rate)


def strengthened(result, key, source, target, blocks, factor):
    owner, partner = [(jnp.arange(result.shape[position]) // (result.shape[position] // blocks)).reshape([-1 if axis == position else 1 for axis in range(result.ndim)]) for position in (source, target)]
    chosen = jax.random.permutation(key, blocks)[partner]
    strong = (owner == chosen) | (owner == (partner + blocks // 2) % blocks)
    return jnp.where(strong, factor * result, result)


def level_of(stream_key, extent, cuts, smallest, high):
    factor_of = 1.0
    for axis_at, shards_of in cuts:
        heights = jax.random.uniform(jax.random.fold_in(jax.random.fold_in(stream_key, 6), axis_at), (shards_of,), jnp.float32, smallest / len(cuts), high / len(cuts))
        factor_of = factor_of * jnp.repeat(jnp.exp(heights), extent[axis_at] // shards_of).reshape((-1,) + (1,) * (len(extent) - 1 - axis_at))
    return factor_of


def gaussian(key, extent, spread, most, pieces=(), held_as=jnp.bfloat16):
    values = jax.random.normal(key, extent, jnp.float32) * spread
    if len(pieces) > 0:
        values = level_of(key, extent, pieces, -0.22, 0.18) * values
    return jnp.clip(values, min=-most, max=most).astype(held_as)


def bell_draw_with(rng, dims, scale, bound, shards, heavy, kind=jnp.bfloat16):
    entries = scale * jax.random.normal(rng, dims, jnp.float32)
    if shards:
        entries = entries * level_of(rng, dims, shards, -0.22, 0.18)
    return jnp.clip(strengthened(entries, jax.random.fold_in(rng, 3), *heavy), -bound, bound).astype(kind)


def setup_inputs(seed: int = 0) -> dict:
    seeds = jax.random.split(jax.random.key(seed), 17)
    return {
        "layer_activity": bell_draw_with(seeds[0], (BATCH_TOTAL, TOKEN_TOTAL, D), 1.0, 6.0, ((0, 4), (1, 8)), (1, 2, 8, 2.0)),
        "writer_matrix": gaussian(seeds[1], (D, GROUPS * STATE), D ** -0.5, 0.125, ((0, 4),)),
        "reader_matrix": gaussian(seeds[2], (D, GROUPS * STATE), D ** -0.5, 0.125, ((0, 4),)),
        "source_unfiltered": gaussian(seeds[3], (BATCH_TOTAL, TOKEN_TOTAL, INNER), 1.0, 6.0, ((0, 4), (1, 8))),
        "switch_raw_signal": gaussian(seeds[4], (BATCH_TOTAL, TOKEN_TOTAL, INNER), 1.0, 6.0, ((0, 4), (1, 8))),
        "saved_result": gaussian(seeds[5], (BATCH_TOTAL, TOKEN_TOTAL, INNER), 1.0, 6.0, ((0, 4), (1, 8))),
        "final_adjoint": gaussian(seeds[6], (BATCH_TOTAL, TOKEN_TOTAL, INNER), 1.0, 6.0, ((0, 4), (1, 8))),
        "delta_raw": draw_delta_raw(jax.random.fold_in(seeds[16], 71), 0),
        "extra_logdrop": draw_extra_logdrop(jax.random.fold_in(seeds[16], 71), 0),
        "source_filter_coefs": gaussian(seeds[9], (CONV_K, INNER), CONV_K ** -0.5, 2.5, ((1, 8),), jnp.float32),
        "writer_filter_coefs": gaussian(seeds[10], (CONV_K, GROUPS * STATE), CONV_K ** -0.5, 2.5, (), jnp.float32),
        "reader_filter_coefs": gaussian(seeds[11], (CONV_K, GROUPS * STATE), CONV_K ** -0.5, 2.5, (), jnp.float32),
        "delta_offset": jnp.clip(-7.5 + 1.5 * jax.random.uniform(seeds[12], (HEADS,), jnp.float32) ** level_of(seeds[12], (HEADS,), ((0, 8),), -0.2, 0.2), -7.5, -6.0),
        "fading_exponents": draw_fading_exponents(jax.random.fold_in(seeds[16], 71), 0),
        "direct_factor": jnp.clip(1.0 + 0.18 * jax.random.normal(seeds[14], (HEADS,), jnp.float32), 0.1, 1.9),
        "rescale_factor": jnp.clip(1.0 + 0.18 * jax.random.normal(seeds[15], (INNER,), jnp.float32), 0.1, 1.9),
    }


EPSILON = 1e-06
highest = lax.Precision.HIGHEST

def centred_conv(values, tap_weights):
    sample_window = values.shape[0]
    reach_side = (tap_weights.shape[0] - 1) // 2
    padded = jnp.pad(values, ((reach_side, reach_side), (0, 0)))
    summed = jnp.zeros_like(values)
    for offset in range(tap_weights.shape[0]):
        summed = summed + tap_weights[offset][None, :] * padded[offset:offset + sample_window]
    return summed

def one_channel_scan(source_unfiltered, writer_unfiltered, reader_unfiltered, delta_raw, extra_logdrop, source_filter_coefs, writer_filter_coefs, reader_filter_coefs, delta_offset, fading_exponents, direct_factor):
    inputs = jax.nn.silu(centred_conv(source_unfiltered, source_filter_coefs))
    keys_b = jax.nn.silu(centred_conv(writer_unfiltered, writer_filter_coefs))
    reads_c = jax.nn.silu(centred_conv(reader_unfiltered, reader_filter_coefs))
    smooth_delta = jax.nn.softplus(delta_raw + delta_offset)
    channel_fading = smooth_delta * jnp.exp(fading_exponents) + extra_logdrop
    cumulative = jnp.cumsum(channel_fading)
    sample_window = source_unfiltered.shape[0]
    blocks = sample_window // BLOCK
    driven = (inputs * smooth_delta[:, None]).reshape(blocks, BLOCK, -1)
    keyed = keys_b.reshape(blocks, BLOCK, -1)
    reading = reads_c.reshape(blocks, BLOCK, -1)
    levels = cumulative.reshape(blocks, BLOCK)
    within = jnp.exp(-jnp.abs(levels[:, :, None] - levels[:, None, :]))
    scores = jnp.einsum('ktn,ksn->kts', reading, keyed, precision=highest) * within
    output = jnp.einsum('kts,ksp->ktp', scores, driven, precision=highest)
    block_ends = levels[:, -1]
    block_starts = levels[:, 0]
    block_order = jnp.arange(blocks, dtype=jnp.int32)
    prev_end = jnp.concatenate([cumulative[:1], block_ends[:-1]])
    next_start = jnp.concatenate([block_starts[1:], cumulative[-1:]])
    weight_fwd = jnp.exp(levels - block_ends[:, None])
    state_fwd = jnp.einsum('ksn,ksp->knp', keyed * weight_fwd[:, :, None], driven, precision=highest)
    mask_fwd = (block_order[None, :] < block_order[:, None]).astype(cumulative.dtype)
    link_fwd = jnp.exp(-jnp.abs(prev_end[:, None] - block_ends[None, :])) * mask_fwd
    carry_fwd = jnp.einsum('kj,jnp->knp', link_fwd, state_fwd, precision=highest)
    read_fwd = reading * jnp.exp(prev_end[:, None] - levels)[:, :, None]
    weight_bwd = jnp.exp(block_starts[:, None] - levels)
    state_bwd = jnp.einsum('ksn,ksp->knp', keyed * weight_bwd[:, :, None], driven, precision=highest)
    mask_bwd = (block_order[None, :] > block_order[:, None]).astype(cumulative.dtype)
    link_bwd = jnp.exp(-jnp.abs(next_start[:, None] - block_starts[None, :])) * mask_bwd
    carry_bwd = jnp.einsum('kj,jnp->knp', link_bwd, state_bwd, precision=highest)
    read_bwd = reading * jnp.exp(levels - next_start[:, None])[:, :, None]
    output = output + jnp.einsum('ktn,knp->ktp', read_fwd, carry_fwd, precision=highest)
    output = output + jnp.einsum('ktn,knp->ktp', read_bwd, carry_bwd, precision=highest)
    return output.reshape(sample_window, -1) + direct_factor * inputs

def channelwise_derivs(source_unfiltered, writer_unfiltered, reader_unfiltered, delta_raw, extra_logdrop, source_filter_coefs, writer_filter_coefs, reader_filter_coefs, delta_offset, fading_exponents, direct_factor, result_adjoint):

    def forward(source_filtered, writer_filtered, reader_filtered, delta_argument):
        return one_channel_scan(source_filtered, writer_filtered, reader_filtered, delta_argument, extra_logdrop, source_filter_coefs, writer_filter_coefs, reader_filter_coefs, delta_offset, fading_exponents, direct_factor)
    primal, pullback = jax.vjp(forward, source_unfiltered.astype(jnp.float32), writer_unfiltered.astype(jnp.float32), reader_unfiltered.astype(jnp.float32), delta_raw.astype(jnp.float32))
    source_derivative, writer_derivative, reader_derivative, delta_derivative = pullback(result_adjoint.astype(jnp.float32))
    return (source_derivative.astype(jnp.bfloat16), writer_derivative.astype(jnp.bfloat16), reader_derivative.astype(jnp.bfloat16), delta_derivative.astype(jnp.bfloat16))

def gated_norm(values, gating, rescale_factor):
    mixed = values * jax.nn.silu(gating)
    grouped = mixed.reshape(mixed.shape[0], NORM_GROUPS, -1)
    scaled = grouped * lax.rsqrt(lax.optimization_barrier(jnp.mean(grouped * grouped, axis=-1, keepdims=True)) + EPSILON)
    return scaled.reshape(mixed.shape) * rescale_factor

def norm_backward(saved_result, switch_raw_signal, final_adjoint, rescale_factor):
    primal, pullback = jax.vjp(lambda values, gating: gated_norm(values, gating, rescale_factor), saved_result.astype(jnp.float32), switch_raw_signal.astype(jnp.float32))
    d_values, d_gates = pullback(final_adjoint.astype(jnp.float32))
    return (d_values.astype(jnp.bfloat16), d_gates.astype(jnp.bfloat16))

def reference(layer_activity, writer_matrix, reader_matrix, source_unfiltered, switch_raw_signal, saved_result, final_adjoint, delta_raw, extra_logdrop, source_filter_coefs, writer_filter_coefs, reader_filter_coefs, delta_offset, fading_exponents, direct_factor, rescale_factor):
    latent_dimension = GROUPS * STATE
    per_group = HEADS // GROUPS
    group_of = jnp.arange(HEADS, dtype=jnp.int32) // per_group
    token_rows = layer_activity.reshape(BATCH_TOTAL * TOKEN_TOTAL, D)
    writer_linear = jnp.dot(token_rows, writer_matrix, preferred_element_type=jnp.float32).astype(jnp.bfloat16)
    reader_linear = jnp.dot(token_rows, reader_matrix, preferred_element_type=jnp.float32).astype(jnp.bfloat16)
    source_filter_fn = jnp.transpose(source_filter_coefs.reshape(CONV_K, HEADS, HEAD_DIM), (1, 0, 2))
    writer_filter_fn = jnp.transpose(writer_filter_coefs.reshape(CONV_K, GROUPS, STATE)[:, group_of], (1, 0, 2))
    reader_filter_fn = jnp.transpose(reader_filter_coefs.reshape(CONV_K, GROUPS, STATE)[:, group_of], (1, 0, 2))

    def one_sample_pass(collected_parts):
        sample_source, sample_writer, sample_reader, sample_delta, sample_logdrop_lines, sample_result, sample_switch, sample_final = collected_parts
        result_adjoint, d_gate = norm_backward(sample_result, sample_switch, sample_final, rescale_factor)
        channelwise_source = jnp.transpose(sample_source.reshape(TOKEN_TOTAL, HEADS, HEAD_DIM), (1, 0, 2))
        channelwise_writer = jnp.transpose(sample_writer.reshape(TOKEN_TOTAL, GROUPS, STATE)[:, group_of], (1, 0, 2))
        channelwise_reader = jnp.transpose(sample_reader.reshape(TOKEN_TOTAL, GROUPS, STATE)[:, group_of], (1, 0, 2))
        channelwise_adjoint = jnp.transpose(result_adjoint.reshape(TOKEN_TOTAL, HEADS, HEAD_DIM), (1, 0, 2))
        source_derivative, writer_derivative, reader_derivative, delta_derivative = lax.map(lambda collected_items: channelwise_derivs(*collected_items), (channelwise_source, channelwise_writer, channelwise_reader, sample_delta.T, sample_logdrop_lines.T, source_filter_fn, writer_filter_fn, reader_filter_fn, delta_offset, fading_exponents, direct_factor, channelwise_adjoint))
        summed_b = lax.optimization_barrier(jnp.sum(writer_derivative.astype(jnp.float32).reshape(GROUPS, per_group, TOKEN_TOTAL, STATE), axis=1))
        summed_c = lax.optimization_barrier(jnp.sum(reader_derivative.astype(jnp.float32).reshape(GROUPS, per_group, TOKEN_TOTAL, STATE), axis=1))
        summed_b = jnp.transpose(summed_b, (1, 0, 2)).reshape(TOKEN_TOTAL, latent_dimension).astype(jnp.bfloat16)
        summed_c = jnp.transpose(summed_c, (1, 0, 2)).reshape(TOKEN_TOTAL, latent_dimension).astype(jnp.bfloat16)
        return (jnp.transpose(source_derivative, (1, 0, 2)).reshape(TOKEN_TOTAL, INNER), summed_b, summed_c, delta_derivative.T, d_gate)
    whole_batch_source, whole_batch_writer, whole_batch_reader, whole_batch_delta, whole_batch_switch = lax.map(one_sample_pass, (source_unfiltered, writer_linear.reshape(BATCH_TOTAL, TOKEN_TOTAL, latent_dimension), reader_linear.reshape(BATCH_TOTAL, TOKEN_TOTAL, latent_dimension), delta_raw, extra_logdrop, saved_result, switch_raw_signal, final_adjoint))
    grad_rows_b = whole_batch_writer.reshape(BATCH_TOTAL * TOKEN_TOTAL, latent_dimension)
    grad_rows_c = whole_batch_reader.reshape(BATCH_TOTAL * TOKEN_TOTAL, latent_dimension)
    d_hidden = (jnp.dot(grad_rows_b, writer_matrix.T, preferred_element_type=jnp.float32) + jnp.dot(grad_rows_c, reader_matrix.T, preferred_element_type=jnp.float32)).astype(jnp.bfloat16)
    d_w_b = jnp.dot(token_rows.T, grad_rows_b, preferred_element_type=jnp.float32)
    d_w_c = jnp.dot(token_rows.T, grad_rows_c, preferred_element_type=jnp.float32)
    return (d_hidden.reshape(BATCH_TOTAL, TOKEN_TOTAL, D), whole_batch_source, whole_batch_switch, whole_batch_delta, d_w_b, d_w_c)
```

```python
import functools

import jax
import jax.numpy as jnp
from jax import lax
from jax.experimental import pallas as pl
from jax.experimental.pallas import tpu as pltpu
from jax.sharding import PartitionSpec as P

HEADS = 32
HEAD_DIM = 64
STATE = 128
GROUPS = 2
NORM_GROUPS = 8
CONV_K = 5
BLOCK = 128
INNER = 2048
EXTRA = 16
ROWS = 8

EPSILON = 1e-06
highest = lax.Precision.HIGHEST
f32 = jnp.float32
bf16 = jnp.bfloat16


def nn(a, b, **kw):
    return lax.dot_general(a, b, (((1,), (0,)), ((), ())), preferred_element_type=f32, **kw)


def nt(a, b, **kw):
    return lax.dot_general(a, b, (((1,), (1,)), ((), ())), preferred_element_type=f32, **kw)


def tn(a, b, **kw):
    return lax.dot_general(a, b, (((0,), (0,)), ((), ())), preferred_element_type=f32, **kw)


def pack_rows(rows, width):
    heads = rows.shape[0]
    if width >= BLOCK:
        per = width // BLOCK
        lines = [
            jnp.concatenate([rows[i * per + j : i * per + j + 1] for j in range(per)], axis=1)
            for i in range(heads // per)
        ]
    else:
        lines = [rows[:, i * width : (i + 1) * width] for i in range(BLOCK // width)]
    spare = EXTRA - sum(line.shape[0] for line in lines)
    return jnp.concatenate(lines + [jnp.zeros((spare, width), rows.dtype)], axis=0)


def unpack_rows(lines, heads, width):
    if width >= BLOCK:
        per = width // BLOCK
        rows = [
            lines[i : i + 1, j * BLOCK : (j + 1) * BLOCK]
            for i in range(heads // per)
            for j in range(per)
        ]
    else:
        rows = [jnp.concatenate([lines[i : i + 1] for i in range(BLOCK // width)], axis=1)]
    return jnp.concatenate(rows + [jnp.zeros((ROWS - heads, BLOCK), lines.dtype)], axis=0)


def pack_kernel(x_ref, dt_ref, out_ref):
    devices, _, width = out_ref.shape
    heads = dt_ref.shape[1] // devices
    dt_rows = dt_ref[...].astype(f32).T
    for i in range(devices):
        out_ref[i, :BLOCK, :] = x_ref[:, i * width : (i + 1) * width]
        out_ref[i, BLOCK:, :] = pack_rows(dt_rows[i * heads : (i + 1) * heads], width).astype(bf16)


def norm_kernel(saved_ref, switch_ref, final_ref, scale_ref, dy_ref, gate_ref):
    values = saved_ref[...].astype(f32)
    switch = switch_ref[...].astype(f32)
    cot = final_ref[...].astype(f32) * scale_ref[...]
    sig = 1.0 / (1.0 + jnp.exp(-switch))
    silu = switch * sig
    g = values * silu
    inv = lax.rsqrt(jnp.mean(g * g, axis=-1, keepdims=True) + EPSILON)
    scaled = g * inv
    d_g = inv * (cot - scaled * jnp.mean(cot * scaled, axis=-1, keepdims=True))
    dy_ref[0] = (d_g * silu).astype(bf16)
    gate_ref[...] = (d_g * values * (sig * (1.0 + switch * (1.0 - sig)))).astype(bf16)


def mixer_kernel(
    x_ref,
    bc_ref,
    dy_ref,
    drop_ref,
    prm_ref,
    skip_ref,
    xw_ref,
    bcw_ref,
    out_ref,
    dbc_ref,
    xpad,
    bcpad,
    u_s,
    us_s,
    k_s,
    r_s,
    kcs_s,
    cum_s,
    dt_s,
    sig_s,
    dec_s,
    duo_s,
    dui_s,
    gi_s,
    go_s,
    sf_s,
    sb_s,
    tf_s,
    tb_s,
):
    blocks, _, width = x_ref.shape
    heads = width // HEAD_DIM
    pad = 8
    it_r = lax.broadcasted_iota(jnp.int32, (BLOCK, BLOCK), 0)
    it_c = lax.broadcasted_iota(jnp.int32, (BLOCK, BLOCK), 1)
    incl = (it_r <= it_c).astype(f32)
    suff = (it_r >= it_c).astype(f32)
    pref = (it_r < it_c).astype(f32)
    expand = (
        lax.broadcasted_iota(jnp.int32, (ROWS, width), 1) // HEAD_DIM
        == lax.broadcasted_iota(jnp.int32, (ROWS, width), 0)
    ).astype(f32)

    xpad[0:pad, :] = jnp.zeros((pad, width), f32)
    xpad[pad + blocks * BLOCK :, :] = jnp.zeros((pad, width), f32)
    bcpad[0:pad, :] = jnp.zeros((pad, 2 * STATE), f32)
    bcpad[pad + blocks * BLOCK :, :] = jnp.zeros((pad, 2 * STATE), f32)

    def load_block(b, _):
        at = pl.multiple_of(b * BLOCK, BLOCK) + pad
        xpad[pl.ds(at, BLOCK), :] = x_ref[b, :BLOCK, :].astype(f32)
        bcpad[pl.ds(at, BLOCK), :] = bc_ref[b].astype(f32)
        return 0

    lax.fori_loop(0, blocks, load_block, 0)

    def conv(pad_ref, b, w_ref, flip):
        win = pad_ref[pl.ds(pl.multiple_of(b * BLOCK, BLOCK), BLOCK + 2 * pad), :]
        total = None
        for k in range(CONV_K):
            shift = (CONV_K - 1) // 2 - k
            moved = win if shift == 0 else pltpu.roll(win, shift % (BLOCK + 2 * pad), 0)
            tap = w_ref[CONV_K - 1 - k : CONV_K - k, :] if flip else w_ref[k : k + 1, :]
            term = moved[pad : pad + BLOCK] * tap
            total = term if total is None else total + term
        return total

    def first(b, _):
        pre = conv(xpad, b, xw_ref, False)
        sig = 1.0 / (1.0 + jnp.exp(-pre))
        u = pre * sig
        u_s[b] = u
        us_s[b] = sig * (1.0 + pre * (1.0 - sig))
        pre = conv(bcpad, b, bcw_ref, False)
        sig = 1.0 / (1.0 + jnp.exp(-pre))
        act = (pre * sig).astype(bf16)
        kcs_s[b] = sig * (1.0 + pre * (1.0 - sig))
        keys = act[:, :STATE]
        reads = act[:, STATE:]
        k_s[b] = keys
        r_s[b] = reads
        raw = unpack_rows(x_ref[b, BLOCK:, :].astype(f32), heads, width) + prm_ref[0]
        dt = jnp.maximum(raw, 0.0) + jnp.log1p(jnp.exp(-jnp.abs(raw)))
        rate = dt * jnp.exp(prm_ref[1]) + drop_ref[b]
        cum = nn(rate, incl, precision=highest)
        total = cum[:, BLOCK - 1 :]
        e_in = jnp.exp(-cum)
        e_out = jnp.exp(cum - total)
        cum_s[b] = cum
        dt_s[b] = dt
        sig_s[b] = 1.0 / (1.0 + jnp.exp(-raw))
        decay = tn(jnp.broadcast_to(jnp.exp(-total), (ROWS, ROWS)), expand, precision=highest)
        dec_s[b] = decay
        wide = tn(jnp.concatenate([dt, e_in, e_out], axis=1), expand, precision=highest)
        driven = u * wide[:BLOCK]
        w_in = wide[BLOCK : 2 * BLOCK]
        w_out = wide[2 * BLOCK :]
        g = dy_ref[b].astype(f32)
        duo = (driven * w_out).astype(bf16)
        dui = (driven * w_in).astype(bf16)
        gi = (g * w_in).astype(bf16)
        go = (g * w_out).astype(bf16)
        duo_s[b] = duo
        dui_s[b] = dui
        gi_s[b] = gi
        go_s[b] = go
        sf_s[b] = tn(keys, duo)
        sb_s[b] = tn(keys, dui)
        tf_s[b] = tn(reads, gi)
        tb_s[b] = tn(reads, go)
        return 0

    lax.fori_loop(0, blocks, first, 0)

    def scan(i, carry):
        f, y, bk, x = carry
        j = blocks - 1 - i
        dec_i = dec_s[i][0:1]
        dec_j = dec_s[j][0:1]
        new = (sf_s[i], tb_s[i], sb_s[j], tf_s[j])
        sf_s[i] = f
        tb_s[i] = y
        sb_s[j] = bk
        tf_s[j] = x
        return (
            f * dec_i + new[0],
            y * dec_i + new[1],
            bk * dec_j + new[2],
            x * dec_j + new[3],
        )

    zero = jnp.zeros((STATE, width), f32)
    lax.fori_loop(0, blocks, scan, (zero, zero, zero, zero))

    ones = jnp.ones((ROWS, BLOCK), bf16)
    row_id = lax.broadcasted_iota(jnp.int32, (ROWS, BLOCK), 0)
    sign = jnp.where(it_r > it_c, 1.0, jnp.where(it_r < it_c, -1.0, 0.0)).astype(f32)

    def second(b, _):
        keys = k_s[b]
        reads = r_s[b]
        u = u_s[b]
        g16 = dy_ref[b]
        cum = cum_s[b]
        dt = dt_s[b]
        cum_t = cum.T
        wide = tn(jnp.concatenate([dt, jnp.exp(-cum), jnp.exp(cum - cum[:, BLOCK - 1 :])], axis=1), expand, precision=highest)
        w_dt = wide[:BLOCK]
        w_in = wide[BLOCK : 2 * BLOCK]
        w_out = wide[2 * BLOCK :]
        driven = (u * w_dt).astype(bf16)
        duo = duo_s[b]
        dui = dui_s[b]
        gi = gi_s[b]
        go = go_s[b]
        carry_f = sf_s[b]
        carry_y = tb_s[b]
        carry_b = sb_s[b]
        carry_x = tf_s[b]
        cf16 = carry_f.astype(bf16)
        cy16 = carry_y.astype(bf16)
        cb16 = carry_b.astype(bf16)
        cx16 = carry_x.astype(bf16)
        y_f = nn(reads, cf16)
        y_b = nn(reads, cb16)
        c_x = nn(keys, cx16)
        c_y = nn(keys, cy16)
        d_r = nt(gi, cf16) + nt(go, cb16)
        d_k = nt(duo, cx16) + nt(dui, cy16)
        scores = nt(keys, reads)
        d_scores = jnp.zeros((BLOCK, BLOCK), f32)
        d_driven = []
        inside = jnp.zeros((ROWS, BLOCK), f32)
        for h in range(heads):
            lo, hi = h * HEAD_DIM, (h + 1) * HEAD_DIM
            decay = jnp.exp(-jnp.abs(cum_t[:, h : h + 1] - cum[h : h + 1, :]))
            gu = nt(driven[:, lo:hi], g16[:, lo:hi])
            s = scores * decay
            d_scores = d_scores + gu * decay
            d_driven.append(nn(s.astype(bf16), g16[:, lo:hi]))
            z = (s * gu * sign).astype(bf16)
            inside = jnp.where(row_id == h, nt(ones, z) - nn(ones, z), inside)
        ds16 = d_scores.astype(bf16)
        d_k = d_k + nn(ds16, reads)
        d_r = d_r + tn(ds16, keys)
        d_dr = jnp.concatenate(d_driven, axis=1) + w_out * c_x + w_in * c_y
        suffix = gi.astype(f32) * y_f + dui.astype(f32) * c_y
        prefix = duo.astype(f32) * c_x + go.astype(f32) * y_b
        through = jnp.sum(carry_f * carry_x + carry_b * carry_y, axis=0, keepdims=True) * dec_s[b][0:1]
        seg = nt(expand, jnp.concatenate([suffix, prefix, d_dr * u, jnp.broadcast_to(through, (ROWS, width))], axis=0), precision=highest)
        d_rate = -(
            nn(seg[:, :BLOCK] + inside, suff, precision=highest)
            + nn(seg[:, BLOCK : 2 * BLOCK], pref, precision=highest)
            + seg[:, 3 * BLOCK : 3 * BLOCK + 1]
        )
        d_dt = (seg[:, 2 * BLOCK : 3 * BLOCK] + d_rate * jnp.exp(prm_ref[1])) * sig_s[b]
        out_ref[b, BLOCK:, :] = pack_rows(d_dt[:heads], width).astype(bf16)
        d_u = d_dr * w_dt + g16.astype(f32) * skip_ref[...]
        at = pl.multiple_of(b * BLOCK, BLOCK) + pad
        xpad[pl.ds(at, BLOCK), :] = d_u * us_s[b]
        bcpad[pl.ds(at, BLOCK), :] = jnp.concatenate([d_k, d_r], axis=1) * kcs_s[b]
        return 0

    lax.fori_loop(0, blocks, second, 0)

    def last(b, _):
        out_ref[b, :BLOCK, :] = conv(xpad, b, xw_ref, True).astype(bf16)
        dbc_ref[b] = conv(bcpad, b, bcw_ref, True).astype(bf16)
        return 0

    lax.fori_loop(0, blocks, last, 0)


def vmem():
    return pl.BlockSpec(memory_space=pltpu.VMEM)


def run_mixer(x, bc, dy, drop, prm, skip, xw, bcw):
    blocks, rows, width = x.shape
    length = blocks * BLOCK
    wide = (blocks, BLOCK, width)
    scratch = [
        pltpu.VMEM((length + 16, width), f32),
        pltpu.VMEM((length + 16, 2 * STATE), f32),
        pltpu.VMEM(wide, f32),
        pltpu.VMEM(wide, f32),
        pltpu.VMEM((blocks, BLOCK, STATE), bf16),
        pltpu.VMEM((blocks, BLOCK, STATE), bf16),
        pltpu.VMEM((blocks, BLOCK, 2 * STATE), f32),
        pltpu.VMEM((blocks, ROWS, BLOCK), f32),
        pltpu.VMEM((blocks, ROWS, BLOCK), f32),
        pltpu.VMEM((blocks, ROWS, BLOCK), f32),
        pltpu.VMEM((blocks, ROWS, width), f32),
        pltpu.VMEM(wide, bf16),
        pltpu.VMEM(wide, bf16),
        pltpu.VMEM(wide, bf16),
        pltpu.VMEM(wide, bf16),
        pltpu.VMEM((blocks, STATE, width), f32),
        pltpu.VMEM((blocks, STATE, width), f32),
        pltpu.VMEM((blocks, STATE, width), f32),
        pltpu.VMEM((blocks, STATE, width), f32),
    ]
    return pl.pallas_call(
        mixer_kernel,
        out_shape=(
            jax.ShapeDtypeStruct((blocks, rows, width), bf16),
            jax.ShapeDtypeStruct((blocks, BLOCK, 2 * STATE), bf16),
        ),
        in_specs=[vmem()] * 8,
        out_specs=(vmem(), vmem()),
        scratch_shapes=scratch,
        name="mixer",
    )(x, bc, dy, drop, prm, skip, xw, bcw)


def exchange(value, axis, groups=None):
    return lax.all_to_all(value, axis, 0, 0, tiled=True, axis_index_groups=groups)


def spread(value, axis, count, groups=None):
    copies = jnp.broadcast_to(value[None], (count,) + value.shape)
    return exchange(copies, axis, groups)


def local(
    layer_activity,
    writer_matrix,
    reader_matrix,
    source_unfiltered,
    switch_raw_signal,
    saved_result,
    final_adjoint,
    delta_raw,
    extra_logdrop,
    source_filter_coefs,
    writer_filter_coefs,
    reader_filter_coefs,
    delta_offset,
    fading_exponents,
    direct_factor,
    rescale_factor,
):
    tokens = layer_activity.shape[1]
    width_in = layer_activity.shape[2]
    dp = lax.axis_size("dp")
    sp = lax.axis_size("sp")
    heads = delta_offset.shape[0]
    width = heads * HEAD_DIM
    per_group = sp // GROUPS
    my_group = lax.axis_index("sp") // per_group
    cols = INNER // NORM_GROUPS

    weights = spread(jnp.concatenate([writer_matrix, reader_matrix], axis=1), "dp", dp)
    weights = weights.reshape(width_in, 2 * GROUPS * STATE)

    packed = pl.pallas_call(
        pack_kernel,
        out_shape=jax.ShapeDtypeStruct((sp, BLOCK + EXTRA, width), bf16),
        in_specs=[vmem(), vmem()],
        out_specs=vmem(),
        name="pack",
    )(source_unfiltered[0], delta_raw[0])
    heads_x = exchange(packed, "sp")

    row_spec = pl.BlockSpec((tokens, cols), lambda i: (0, i))
    d_y, d_gate = pl.pallas_call(
        norm_kernel,
        grid=(NORM_GROUPS,),
        in_specs=[row_spec, row_spec, row_spec, pl.BlockSpec((1, cols), lambda i: (0, i))],
        out_specs=(pl.BlockSpec((1, tokens, cols), lambda i: (i, 0, 0)), row_spec),
        out_shape=(
            jax.ShapeDtypeStruct((NORM_GROUPS, tokens, cols), bf16),
            jax.ShapeDtypeStruct((tokens, INNER), bf16),
        ),
        name="norm",
    )(saved_result[0], switch_raw_signal[0], final_adjoint[0], rescale_factor[None])
    if cols != width:
        d_y = d_y.transpose(1, 0, 2).reshape(tokens, sp, width).transpose(1, 0, 2)
    heads_dy = exchange(d_y, "sp")

    rows = layer_activity[0]
    projected = jnp.dot(rows, weights, preferred_element_type=f32).astype(bf16)
    by_group = projected.reshape(tokens, 2, GROUPS, STATE)
    by_group = by_group.transpose(2, 0, 1, 3).reshape(GROUPS, 1, tokens, 2 * STATE)
    copies = jnp.broadcast_to(by_group, (GROUPS, per_group, tokens, 2 * STATE))
    heads_bc = exchange(copies.reshape(sp, tokens, 2 * STATE), "sp")

    blocks = heads_x.shape[0]
    drop = jnp.pad(
        extra_logdrop[0].reshape(blocks, BLOCK, heads).transpose(0, 2, 1),
        ((0, 0), (0, ROWS - heads), (0, 0)),
    )
    prm = jnp.pad(jnp.stack([delta_offset, fading_exponents]), ((0, 0), (0, ROWS - heads)))
    prm = jnp.broadcast_to(prm[:, :, None], (2, ROWS, BLOCK))
    skip = jnp.repeat(direct_factor, HEAD_DIM)[None]
    bcw = jnp.stack([writer_filter_coefs, reader_filter_coefs], axis=1)
    bcw = bcw.reshape(CONV_K, 2, GROUPS, STATE)
    bcw = lax.dynamic_index_in_dim(bcw, my_group, 2, keepdims=False).reshape(CONV_K, 2 * STATE)

    d_x, d_bc = run_mixer(heads_x, heads_bc, heads_dy, drop, prm, skip, source_filter_coefs, bcw)

    back_bc = exchange(d_bc, "sp")
    back_x = exchange(d_x, "sp")

    summed = jnp.sum(
        back_bc.reshape(GROUPS, per_group, tokens, 2, STATE).astype(f32), axis=1
    ).astype(bf16)
    gradients = summed.transpose(1, 2, 0, 3).reshape(tokens, 2 * GROUPS * STATE)

    blocks_in = rows.reshape(tokens, dp, width_in // dp).transpose(1, 0, 2)
    all_columns = exchange(blocks_in, "dp").reshape(dp * tokens, width_in // dp)
    all_grads = spread(gradients, "dp", dp).reshape(dp * tokens, 2 * GROUPS * STATE)
    local_rows = jnp.einsum("td,tc->dc", all_columns, all_grads, preferred_element_type=f32)

    half = sp // 2
    groups = [list(range(half)), list(range(half, sp))]
    shard_rows = local_rows.shape[0] // half
    parts = local_rows.astype(bf16).reshape(half, shard_rows, local_rows.shape[1])
    parts = exchange(parts, "sp", groups)
    mine = jnp.sum(parts.astype(f32), axis=0).astype(bf16)
    other = lax.ppermute(mine, "sp", [(i, (i + half) % sp) for i in range(sp)])
    both = (mine.astype(f32) + other.astype(f32)).astype(bf16)
    total = spread(both, "sp", half, groups).reshape(local_rows.shape).astype(f32)

    d_hidden = jnp.einsum("tc,dc->td", gradients, weights, preferred_element_type=f32).astype(bf16)
    back_dx = back_x[:, :BLOCK].transpose(1, 0, 2).reshape(1, tokens, INNER)
    lines = heads * BLOCK // width
    back_dt = back_x[:, BLOCK : BLOCK + lines].reshape(HEADS, BLOCK).T[None]
    return (
        d_hidden[None],
        back_dx,
        d_gate[None],
        back_dt,
        total[:, : GROUPS * STATE],
        total[:, GROUPS * STATE :],
    )


def solution(mesh):
    in_specs = (
        P("dp", "sp", None),
        P("dp", None),
        P("dp", None),
        P("dp", "sp", None),
        P("dp", "sp", None),
        P("dp", "sp", None),
        P("dp", "sp", None),
        P("dp", "sp", None),
        P("dp", None, "sp"),
        P(None, "sp"),
        P(),
        P(),
        P("sp"),
        P("sp"),
        P("sp"),
        P(),
    )
    out_specs = (
        P("dp", "sp", None),
        P("dp", "sp", None),
        P("dp", "sp", None),
        P("dp", "sp", None),
        P("dp", None),
        P("dp", None),
    )
    return jax.shard_map(local, mesh=mesh, in_specs=in_specs, out_specs=out_specs, check_vma=False)
```

```python
import functools

import jax
import jax.numpy as jnp
from jax import lax
from jax.experimental import pallas as pl
from jax.experimental.pallas import tpu as pltpu
from jax.sharding import PartitionSpec as P


HEADS = 32
HEAD_DIM = 64
STATE = 128
GROUPS = 2
NORM_GROUPS = 8
CONV_K = 5
BLOCK = 128
INNER = 2048
EXTRA = 16
ROWS = 8

EPSILON = 1e-06
f32 = jnp.float32
bf16 = jnp.bfloat16


def nn(a, b, **kw):
    return lax.dot_general(a, b, (((1,), (0,)), ((), ())), preferred_element_type=f32, **kw)


def nt(a, b, **kw):
    return lax.dot_general(a, b, (((1,), (1,)), ((), ())), preferred_element_type=f32, **kw)


def tn(a, b, **kw):
    return lax.dot_general(a, b, (((0,), (0,)), ((), ())), preferred_element_type=f32, **kw)


def pack_rows(rows, width):
    heads = rows.shape[0]
    if width >= BLOCK:
        per = width // BLOCK
        lines = [
            jnp.concatenate([rows[i * per + j : i * per + j + 1] for j in range(per)], axis=1)
            for i in range(heads // per)
        ]
    else:
        lines = [rows[:, i * width : (i + 1) * width] for i in range(BLOCK // width)]
    spare = EXTRA - sum(line.shape[0] for line in lines)
    return jnp.concatenate(lines + [jnp.zeros((spare, width), rows.dtype)], axis=0)


def unpack_rows(lines, heads, width):
    if width >= BLOCK:
        per = width // BLOCK
        rows = [
            lines[i : i + 1, j * BLOCK : (j + 1) * BLOCK]
            for i in range(heads // per)
            for j in range(per)
        ]
    else:
        rows = [jnp.concatenate([lines[i : i + 1] for i in range(BLOCK // width)], axis=1)]
    return jnp.concatenate(rows + [jnp.zeros((ROWS - heads, BLOCK), lines.dtype)], axis=0)


def prep_kernel(saved_ref, switch_ref, final_ref, scale_ref, x_ref, dt_ref, out_ref, gate_ref):
    chunks, _, width = out_ref.shape
    cols = INNER // NORM_GROUPS
    heads = width // HEAD_DIM
    first_row = pl.program_id(0) * chunks * heads
    row = lax.broadcasted_iota(jnp.int32, (max(ROWS, chunks * heads), HEADS), 0)
    pick = (lax.broadcasted_iota(jnp.int32, row.shape, 1) == row + first_row).astype(bf16)
    dt_rows = nt(pick, dt_ref[...])
    for n in range(saved_ref.shape[1] // cols):
        at = slice(n * cols, (n + 1) * cols)
        values = saved_ref[:, at].astype(f32)
        switch = switch_ref[:, at].astype(f32)
        cot = final_ref[:, at].astype(f32) * scale_ref[:, at]
        sig = 1.0 / (1.0 + jnp.exp(-switch))
        silu = switch * sig
        g = values * silu
        inv = lax.rsqrt(jnp.mean(g * g, axis=-1, keepdims=True) + EPSILON)
        scaled = g * inv
        d_g = inv * (cot - scaled * jnp.mean(cot * scaled, axis=-1, keepdims=True))
        d_y = (d_g * silu).astype(bf16)
        gate_ref[:, at] = (d_g * values * (sig * (1.0 + switch * (1.0 - sig)))).astype(bf16)
        for c in range(cols // width):
            i = n * (cols // width) + c
            out_ref[i, :BLOCK, :] = x_ref[:, i * width : (i + 1) * width]
            out_ref[i, BLOCK : 2 * BLOCK, :] = d_y[:, c * width : (c + 1) * width]
            out_ref[i, 2 * BLOCK :, :] = pack_rows(
                dt_rows[i * heads : (i + 1) * heads], width
            ).astype(bf16)


def proj_kernel(at_ref, act_ref, *refs):
    count = len(refs) - 2
    own_ref, other_ref = refs[count:]
    size = act_ref.shape[1] // count
    total = jnp.zeros((act_ref.shape[0], refs[0].shape[1]), f32)
    for k in range(count):
        start = pl.multiple_of((at_ref[0] ^ k) * size, size)
        total = total + nn(act_ref[:, pl.ds(start, size)], refs[k][...])
    wide = total.shape[1] // GROUPS
    low = total[:, :wide].astype(bf16)
    high = total[:, wide:].astype(bf16)
    is_low = jnp.broadcast_to(at_ref[2], low.shape) == 0
    own_ref[...] = jnp.where(is_low, low, high)
    other_ref[...] = jnp.where(is_low, high, low)


def hidden_kernel(at_ref, own_ref, other_ref, *refs):
    count = len(refs) - 1
    out_ref = refs[count]
    size = out_ref.shape[1] // count
    own = own_ref[...]
    other = other_ref[...]
    is_low = jnp.broadcast_to(at_ref[2], own.shape) == 0
    both = jnp.concatenate(
        [jnp.where(is_low, own, other), jnp.where(is_low, other, own)], axis=1
    )
    for k in range(count):
        start = pl.multiple_of((at_ref[0] ^ k) * size, size)
        out_ref[:, pl.ds(start, size)] = nt(both, refs[k][...]).astype(bf16)


def weight_kernel(dp, at_ref, *refs):
    grad_refs = refs[:dp]
    act_refs = refs[dp : 3 * dp]
    out_refs = refs[3 * dp : -1]
    total_ref = refs[-1]
    total = None
    for k in range(dp):
        for part in range(2):
            term = tn(act_refs[part * dp + k][...], grad_refs[k][part])
            total = term if total is None else total + term
    total_ref[...] = total
    size = out_refs[0].shape[0]
    for k, out_ref in enumerate(out_refs):
        start = pl.multiple_of((at_ref[3] ^ k) * size, size)
        out_ref[...] = total_ref[pl.ds(start, size), :].astype(bf16)


def spread_kernel(half, at_ref, *refs):
    outs = refs[2 * half :]
    size = refs[0].shape[0]
    for part in range(2):
        group = at_ref[2] if part == 0 else 1 - at_ref[2]
        lanes = pl.ds(pl.multiple_of(group * STATE, STATE), STATE)
        for k in range(half):
            rows = pl.ds(pl.multiple_of((at_ref[3] ^ k) * size, size), size)
            chunk = refs[part * half + k][...].astype(f32)
            outs[0][rows, lanes] = chunk[:, :STATE]
            outs[1][rows, lanes] = chunk[:, STATE:]


def unpack_kernel(back_ref, dx_ref, dt_ref):
    devices, _, width = back_ref.shape
    heads = width // HEAD_DIM
    rows = []
    for i in range(devices):
        dx_ref[:, i * width : (i + 1) * width] = back_ref[i, :BLOCK, :]
        rows.append(unpack_rows(back_ref[i, BLOCK:, :].astype(f32), heads, width)[:heads])
    dt_ref[...] = jnp.concatenate(rows, axis=0).T.astype(bf16)


def mixer_kernel(
    devices,
    at_ref,
    x_ref,
    drop_ref,
    prm_ref,
    skip_ref,
    xw_ref,
    bcw_ref,
    *refs,
):
    bc_refs = refs[:devices]
    out_ref = refs[devices]
    dbc_refs = refs[devices + 1 : devices + 1 + devices // 2]
    mixer_body(at_ref, x_ref, drop_ref, prm_ref, skip_ref, xw_ref, bcw_ref, bc_refs, out_ref, dbc_refs, *refs[devices + 1 + devices // 2 :])


def split(value, count):
    terms = []
    for _ in range(count):
        terms.append(value.astype(bf16))
        value = value - terms[-1].astype(f32)
    return terms


def mixer_body(
    at_ref,
    x_ref,
    drop_ref,
    prm_ref,
    skip_ref,
    xw_ref,
    bcw_ref,
    bc_refs,
    out_ref,
    dbc_refs,
    xpad,
    bcpad,
    u_s,
    us_s,
    kcs_s,
    kr_s,
    row_s,
    wide_s,
    dr_s,
    gg_s,
    st_s,
    car_s,
    sel_s,
):
    blocks, _, width = x_ref.shape
    heads = width // HEAD_DIM
    pad = 8
    lanes = min(width, BLOCK)
    per = lanes // HEAD_DIM
    all_rows = blocks * ROWS

    def triangle(include):
        r = lax.broadcasted_iota(jnp.int32, (BLOCK, BLOCK), 0)
        c = lax.broadcasted_iota(jnp.int32, (BLOCK, BLOCK), 1)
        return jnp.where(include(r, c), 1.0, 0.0).astype(bf16)

    def expand(count):
        shape = (count * ROWS, width)
        r = lax.broadcasted_iota(jnp.int32, shape, 0) % ROWS
        c = lax.broadcasted_iota(jnp.int32, shape, 1) // HEAD_DIM
        return jnp.where(r == c, 1.0, 0.0)

    r = lax.broadcasted_iota(jnp.int32, (5 * width, BLOCK), 0)
    c = lax.broadcasted_iota(jnp.int32, (5 * width, BLOCK), 1)
    base = jnp.where(r < 2 * width, 0, jnp.where(r < 4 * width, ROWS, 2 * ROWS))
    sel_s[...] = jnp.where(c == base + (r % width) // HEAD_DIM, 1.0, 0.0).astype(bf16)

    xpad[0:pad, :] = jnp.zeros((pad, width), f32)
    xpad[pad + blocks * BLOCK :, :] = jnp.zeros((pad, width), f32)
    bcpad[0:pad, :] = jnp.zeros((pad, 2 * STATE), f32)
    bcpad[pad + blocks * BLOCK :, :] = jnp.zeros((pad, 2 * STATE), f32)

    def load_block(b, _):
        at = pl.multiple_of(b * BLOCK, BLOCK) + pad
        xpad[pl.ds(at, BLOCK), :] = x_ref[b, :BLOCK, :].astype(f32)
        row_s[0, b] = unpack_rows(x_ref[b, 2 * BLOCK :, :].astype(f32), heads, width) + prm_ref[0]
        return 0

    lax.fori_loop(0, blocks, load_block, 0)
    for k, bc_ref in enumerate(bc_refs):
        at = pl.multiple_of((at_ref[1] ^ k) * BLOCK, BLOCK) + pad
        bcpad[pl.ds(at, BLOCK), :] = bc_ref[...].astype(f32)

    raw = row_s[0].reshape(all_rows, BLOCK)
    dt = jnp.maximum(raw, 0.0) + jnp.log1p(jnp.exp(-jnp.abs(raw)))
    fade = jnp.exp(prm_ref[1])
    rate = (dt.reshape(blocks, ROWS, BLOCK) * fade[None] + drop_ref[...]).reshape(all_rows, BLOCK)
    sums = nn(jnp.concatenate(split(rate, 3), axis=0), triangle(lambda r, c: r <= c))
    cum = sums[:all_rows] + sums[all_rows : 2 * all_rows] + sums[2 * all_rows :]
    total = cum[:, BLOCK - 1 :]
    row_s[0] = dt.reshape(blocks, ROWS, BLOCK)
    row_s[1] = cum.reshape(blocks, ROWS, BLOCK)
    row_s[2] = jnp.exp(-cum).reshape(blocks, ROWS, BLOCK)
    row_s[3] = jnp.exp(cum - total).reshape(blocks, ROWS, BLOCK)
    row_s[4] = (1.0 / (1.0 + jnp.exp(-raw))).reshape(blocks, ROWS, BLOCK)

    def conv(pad_ref, b, w_ref, flip):
        win = pad_ref[pl.ds(pl.multiple_of(b * BLOCK, BLOCK), BLOCK + 2 * pad), :]
        total = None
        for k in range(CONV_K):
            shift = (CONV_K - 1) // 2 - k
            moved = win if shift == 0 else pltpu.roll(win, shift % (BLOCK + 2 * pad), 0)
            tap = w_ref[CONV_K - 1 - k : CONV_K - k, :] if flip else w_ref[k : k + 1, :]
            term = moved[pad : pad + BLOCK] * tap
            total = term if total is None else total + term
        return total

    def first(b, _):
        pre = conv(bcpad, b, bcw_ref, False)
        sig = 1.0 / (1.0 + jnp.exp(-pre))
        act = (pre * sig).astype(bf16)
        kcs_s[b] = sig * (1.0 + pre * (1.0 - sig))
        kr_s[b] = act
        pre = conv(xpad, b, xw_ref, False)
        sig = 1.0 / (1.0 + jnp.exp(-pre))
        u = pre * sig
        u_s[b] = u
        us_s[b] = sig * (1.0 + pre * (1.0 - sig))
        rows = jnp.concatenate([row_s[0, b], row_s[2, b], row_s[3, b]], axis=1)
        wide = tn(jnp.concatenate(split(rows, 3), axis=0), expand(3).astype(bf16))
        wide_s[b] = wide
        w_in = wide[BLOCK : 2 * BLOCK]
        w_out = wide[2 * BLOCK :]
        driven = u * wide[:BLOCK]
        g = x_ref[b, BLOCK : 2 * BLOCK, :].astype(f32)
        d_io = jnp.concatenate([driven * w_out, driven * w_in], axis=1).astype(bf16)
        g_io = jnp.concatenate([g * w_in, g * w_out], axis=1).astype(bf16)
        dr_s[b] = d_io
        gg_s[b] = g_io
        st_s[b, :, : 2 * width] = tn(act[:, :STATE], d_io)
        st_s[b, :, 2 * width :] = tn(act[:, STATE:], g_io)
        return 0

    lax.fori_loop(0, blocks, first, 0)

    def scan(slot, back):
        def step(i, carry):
            b = blocks - 1 - i if back else i
            at = slice(slot * width, (slot + 1) * width)
            car_s[b, :, at] = carry.astype(bf16)
            decay = wide_s[b][2 * BLOCK - 1 : 2 * BLOCK]
            return carry * decay + st_s[b, :, at]

        lax.fori_loop(0, blocks, step, jnp.zeros((STATE, width), f32))

    scan(0, False)
    scan(1, True)
    scan(2, True)
    scan(3, False)

    def second(b, _):
        act = kr_s[b]
        keys = act[:, :STATE]
        reads = act[:, STATE:]
        u = u_s[b]
        g16 = x_ref[b, BLOCK : 2 * BLOCK, :]
        cum = row_s[1, b]
        cum_t = cum.T
        wide = wide_s[b]
        w_dt = wide[:BLOCK]
        w_in = wide[BLOCK : 2 * BLOCK]
        w_out = wide[2 * BLOCK :]
        driven = (u * w_dt).astype(bf16)
        d_io = dr_s[b]
        g_io = gg_s[b]
        carry = car_s[b]
        c_s = carry[:, : 2 * width]
        c_g = carry[:, 2 * width :]
        y = nn(reads, c_s)
        c = nn(keys, c_g)
        d_r = nt(g_io, c_s)
        d_k = nt(d_io, c_g)
        scores = nt(keys, reads)
        upper = lax.broadcasted_iota(jnp.int32, (BLOCK, BLOCK), 0) > lax.broadcasted_iota(
            jnp.int32, (BLOCK, BLOCK), 1
        )
        lane = lax.broadcasted_iota(jnp.int32, (BLOCK, lanes), 1) // HEAD_DIM
        column = lax.broadcasted_iota(jnp.int32, (BLOCK, BLOCK), 1)
        row = lax.broadcasted_iota(jnp.int32, (ROWS, BLOCK), 0)
        d_scores = None
        d_driven = []
        by_key = jnp.zeros((BLOCK, BLOCK), f32)
        by_read = jnp.zeros((ROWS, BLOCK), f32)
        none = jnp.zeros((BLOCK, lanes), bf16)
        for p in range(width // lanes):
            at = slice(p * lanes, (p + 1) * lanes)
            g_p = g16[:, at]
            d_p = driven[:, at]
            gu = nt(
                jnp.concatenate([jnp.where(lane == j, d_p, none) for j in range(per)], axis=0), g_p
            )
            s_p = []
            for j in range(per):
                h = p * per + j
                decay = jnp.exp(-jnp.abs(cum_t[:, h : h + 1] - cum[h : h + 1, :]))
                gu_h = gu[j * BLOCK : (j + 1) * BLOCK]
                s = scores * decay
                term = gu_h * decay
                d_scores = term if d_scores is None else d_scores + term
                z = s * gu_h
                z = jnp.where(upper, z, -z)
                by_key = jnp.where(column == h, jnp.sum(z, axis=1, keepdims=True), by_key)
                by_read = jnp.where(row == h, jnp.sum(z, axis=0, keepdims=True), by_read)
                s_p.append(s.astype(bf16))
            d_driven.append(
                nn(
                    jnp.concatenate(s_p, axis=1),
                    jnp.concatenate([jnp.where(lane == j, g_p, none) for j in range(per)], axis=0),
                )
            )
        ds16 = d_scores.astype(bf16)
        d_k = d_k + nn(ds16, reads)
        d_r = d_r + tn(ds16, keys)
        c_x = c[:, :width]
        c_y = c[:, width:]
        d_dr = jnp.concatenate(d_driven, axis=1) + w_out * c_x + w_in * c_y
        prefix = d_io[:, :width].astype(f32) * c_x + g_io[:, width:].astype(f32) * y[:, width:]
        suffix = g_io[:, :width].astype(f32) * y[:, :width] + d_io[:, width:].astype(f32) * c_y
        sums = nn(
            jnp.concatenate(
                split(suffix - prefix, 2) + split(prefix, 2) + [(d_dr * u).astype(bf16)], axis=1
            ),
            sel_s[...],
        )
        sums = sums.T
        by_key = by_key.T
        through = jnp.sum(c_s.astype(f32) * c_g.astype(f32), axis=0, keepdims=True)
        through = (through[:, :width] + through[:, width:]) * wide[2 * BLOCK - 1 : 2 * BLOCK]
        through = jnp.sum(expand(1) * through, axis=1, keepdims=True)
        before = jnp.sum(sums[ROWS : 2 * ROWS], axis=1, keepdims=True) + through
        row_s[5, b] = sums[:ROWS] + by_key[:ROWS] - by_read
        row_s[2, b] = jnp.broadcast_to(before, (ROWS, BLOCK))
        row_s[3, b] = sums[2 * ROWS : 3 * ROWS]
        d_u = d_dr * w_dt + g16.astype(f32) * skip_ref[...]
        at = pl.multiple_of(b * BLOCK, BLOCK) + pad
        xpad[pl.ds(at, BLOCK), :] = d_u * us_s[b]
        bcpad[pl.ds(at, BLOCK), :] = jnp.concatenate([d_k, d_r], axis=1) * kcs_s[b]
        return 0

    lax.fori_loop(0, blocks, second, 0)

    sums = nn(
        jnp.concatenate(split(row_s[5].reshape(all_rows, BLOCK), 3), axis=0),
        triangle(lambda r, c: r >= c),
    )
    sums = sums[:all_rows] + sums[all_rows : 2 * all_rows] + sums[2 * all_rows :]
    d_rate = -(sums.reshape(blocks, ROWS, BLOCK) + row_s[2])
    row_s[0] = (row_s[3] + d_rate * fade[None]) * row_s[4]

    for k, dbc_ref in enumerate(dbc_refs):
        for part in range(2):
            b = at_ref[1] ^ k if part == 0 else at_ref[1] ^ k ^ len(dbc_refs)
            dbc_ref[part] = conv(bcpad, b, bcw_ref, True).astype(bf16)

    def last(b, _):
        out_ref[b, :BLOCK, :] = conv(xpad, b, xw_ref, True).astype(bf16)
        out_ref[b, BLOCK:, :] = pack_rows(row_s[0, b][:heads], width).astype(bf16)
        return 0

    lax.fori_loop(0, blocks, last, 0)


def vmem():
    return pl.BlockSpec(memory_space=pltpu.VMEM)


def smem():
    return pl.BlockSpec(memory_space=pltpu.SMEM)


def run_mixer(at, x, drop, prm, skip, xw, bcw, bc):
    blocks, _, width = x.shape
    length = blocks * BLOCK
    scratch = [
        pltpu.VMEM((length + 16, width), f32),
        pltpu.VMEM((length + 16, 2 * STATE), f32),
        pltpu.VMEM((blocks, BLOCK, width), f32),
        pltpu.VMEM((blocks, BLOCK, width), f32),
        pltpu.VMEM((blocks, BLOCK, 2 * STATE), f32),
        pltpu.VMEM((blocks, BLOCK, 2 * STATE), bf16),
        pltpu.VMEM((6, blocks, ROWS, BLOCK), f32),
        pltpu.VMEM((blocks, 3 * BLOCK, width), f32),
        pltpu.VMEM((blocks, BLOCK, 2 * width), bf16),
        pltpu.VMEM((blocks, BLOCK, 2 * width), bf16),
        pltpu.VMEM((blocks, STATE, 4 * width), f32),
        pltpu.VMEM((blocks, STATE, 4 * width), bf16),
        pltpu.VMEM((5 * width, BLOCK), bf16),
    ]
    half = len(bc) // 2
    outs = pl.pallas_call(
        functools.partial(mixer_kernel, len(bc)),
        out_shape=(jax.ShapeDtypeStruct((blocks, BLOCK + EXTRA, width), bf16),)
        + (jax.ShapeDtypeStruct((2, BLOCK, 2 * STATE), bf16),) * half,
        in_specs=[smem()] + [vmem()] * (6 + len(bc)),
        out_specs=(vmem(),) * (1 + half),
        scratch_shapes=scratch,
        name="mixer",
    )(at, x, drop, prm, skip, xw, bcw, *bc)
    return outs[0], outs[1:]


def swap(value, axis, bits):
    size = lax.axis_size(axis)
    return lax.ppermute(value, axis, [(i, i ^ bits) for i in range(size)])


def call(kernel, outs, *args, scratch=()):
    specs = [smem()] + [vmem()] * (len(args) - 1)
    return pl.pallas_call(
        kernel,
        out_shape=outs,
        in_specs=specs,
        out_specs=jax.tree.map(lambda _: vmem(), outs),
        scratch_shapes=scratch,
    )(*args)


def local(
    layer_activity,
    writer_matrix,
    reader_matrix,
    source_unfiltered,
    switch_raw_signal,
    saved_result,
    final_adjoint,
    delta_raw,
    extra_logdrop,
    source_filter_coefs,
    writer_filter_coefs,
    reader_filter_coefs,
    delta_offset,
    fading_exponents,
    direct_factor,
    rescale_factor,
):
    tokens = layer_activity.shape[1]
    width_in = layer_activity.shape[2]
    dp = lax.axis_size("dp")
    sp = lax.axis_size("sp")
    half = sp // 2
    heads = delta_offset.shape[0]
    width = heads * HEAD_DIM
    me_d = lax.axis_index("dp")
    me_s = lax.axis_index("sp")
    at = jnp.stack([me_d, me_s, me_s // half, me_s % half]).astype(jnp.int32)
    shape = jax.ShapeDtypeStruct
    rows = layer_activity[0]
    share = width_in // dp

    weights = jnp.concatenate(
        [
            m[:, g * STATE : (g + 1) * STATE]
            for g in range(GROUPS)
            for m in (writer_matrix, reader_matrix)
        ],
        axis=1,
    )
    pieces = {0: weights}
    bit = dp // 2
    while bit:
        pieces.update({k ^ bit: swap(v, "dp", bit) for k, v in list(pieces.items())})
        bit //= 2
    pieces = [pieces[k] for k in range(dp)]

    steps = NORM_GROUPS // 2
    wide = INNER // steps
    row_spec = pl.BlockSpec((tokens, wide), lambda i: (0, i))
    packed, d_gate = pl.pallas_call(
        prep_kernel,
        grid=(steps,),
        in_specs=[
            row_spec,
            row_spec,
            row_spec,
            pl.BlockSpec((1, wide), lambda i: (0, i)),
            row_spec,
            pl.BlockSpec((tokens, HEADS), lambda i: (0, 0)),
        ],
        out_specs=(
            pl.BlockSpec((sp // steps, 2 * BLOCK + EXTRA, width), lambda i: (i, 0, 0)),
            row_spec,
        ),
        out_shape=(
            shape((sp, 2 * BLOCK + EXTRA, width), bf16),
            shape((tokens, INNER), bf16),
        ),
        name="prep",
    )(
        saved_result[0],
        switch_raw_signal[0],
        final_adjoint[0],
        rescale_factor[None],
        source_unfiltered[0],
        delta_raw[0],
    )
    heads_x = lax.all_to_all(packed, "sp", 0, 0, tiled=True)

    acts = [lax.dynamic_slice(rows, (0, (me_d ^ k) * share), (tokens, share)) for k in range(dp)]
    acts = [acts[0]] + [swap(acts[k], "dp", k) for k in range(1, dp)]
    for k in range(dp):
        acts.append(swap(acts[k], "sp", half))

    bc = shape((tokens, 2 * STATE), bf16)
    own, other = call(proj_kernel, (bc, bc), at, rows, *pieces)
    other = swap(other, "sp", half)
    all_bc = [own if k == 0 else swap(own, "sp", k) for k in range(half)]
    all_bc += [other if k == 0 else swap(other, "sp", k) for k in range(half)]

    blocks = heads_x.shape[0]
    drop = jnp.pad(
        extra_logdrop[0].reshape(blocks, BLOCK, heads).transpose(0, 2, 1),
        ((0, 0), (0, ROWS - heads), (0, 0)),
    )
    prm = jnp.pad(jnp.stack([delta_offset, fading_exponents]), ((0, 0), (0, ROWS - heads)))
    prm = jnp.broadcast_to(prm[:, :, None], (2, ROWS, BLOCK))
    skip = jnp.repeat(direct_factor, HEAD_DIM)[None]
    bcw = jnp.stack([writer_filter_coefs, reader_filter_coefs], axis=1)
    bcw = bcw.reshape(CONV_K, 2, GROUPS, STATE)
    bcw = lax.dynamic_index_in_dim(bcw, at[2], 2, keepdims=False).reshape(CONV_K, 2 * STATE)

    d_x, d_bc = run_mixer(at, heads_x, drop, prm, skip, source_filter_coefs, bcw, all_bc)

    parts = [d_bc[0]] + [swap(d_bc[k], "sp", k) for k in range(1, half)]
    grads = functools.reduce(jnp.add, [p.astype(f32) for p in parts]).astype(bf16)
    back_x = lax.all_to_all(d_x, "sp", 0, 0, tiled=True)
    all_grads = [grads if k == 0 else swap(grads, "dp", k) for k in range(dp)]
    rest = swap(grads[1], "sp", half)

    chunk = shape((share // half, 2 * STATE), bf16)
    chunks = call(
        functools.partial(weight_kernel, dp),
        (chunk,) * half,
        at,
        *all_grads,
        *acts,
        scratch=[pltpu.VMEM((share, 2 * STATE), f32)],
    )
    chunks = [chunks[0]] + [swap(chunks[k], "sp", k) for k in range(1, half)]
    mine = functools.reduce(jnp.add, [c.astype(f32) for c in chunks]).astype(bf16)
    theirs = swap(mine, "sp", half)
    placed = [mine if k == 0 else swap(mine, "sp", k) for k in range(half)]
    placed += [theirs if k == 0 else swap(theirs, "sp", k) for k in range(half)]

    d_hidden = call(hidden_kernel, shape((tokens, width_in), bf16), at, grads[0], rest, *pieces)
    d_source, d_delta = pl.pallas_call(
        unpack_kernel,
        out_shape=(shape((tokens, INNER), bf16), shape((tokens, HEADS), bf16)),
        in_specs=[vmem()],
        out_specs=(vmem(), vmem()),
        name="unpack",
    )(back_x)
    matrix = shape((share, GROUPS * STATE), f32)
    d_w_b, d_w_c = call(functools.partial(spread_kernel, half), (matrix, matrix), at, *placed)
    return d_hidden[None], d_source[None], d_gate[None], d_delta[None], d_w_b, d_w_c


def solution(mesh):
    in_specs = (
        P("dp", "sp", None),
        P("dp", None),
        P("dp", None),
        P("dp", "sp", None),
        P("dp", "sp", None),
        P("dp", "sp", None),
        P("dp", "sp", None),
        P("dp", "sp", None),
        P("dp", None, "sp"),
        P(None, "sp"),
        P(),
        P(),
        P("sp"),
        P("sp"),
        P("sp"),
        P(),
    )
    out_specs = (
        P("dp", "sp", None),
        P("dp", "sp", None),
        P("dp", "sp", None),
        P("dp", "sp", None),
        P("dp", None),
        P("dp", None),
    )

    return jax.shard_map(local, mesh=mesh, in_specs=in_specs, out_specs=out_specs, check_vma=False)
```

```python
import functools

import jax
import jax.numpy as jnp
from jax import lax
from jax.experimental import pallas as pl
from jax.experimental.pallas import tpu as pltpu
from jax.sharding import PartitionSpec as P


HEADS = 32
HEAD_DIM = 64
STATE = 128
GROUPS = 2
NORM_GROUPS = 8
CONV_K = 5
BLOCK = 128
INNER = 2048
EXTRA = 16
ROWS = 8

EPSILON = 1e-06
f32 = jnp.float32
bf16 = jnp.bfloat16


def nn(a, b, **kw):
    return lax.dot_general(a, b, (((1,), (0,)), ((), ())), preferred_element_type=f32, **kw)


def nt(a, b, **kw):
    return lax.dot_general(a, b, (((1,), (1,)), ((), ())), preferred_element_type=f32, **kw)


def tn(a, b, **kw):
    return lax.dot_general(a, b, (((0,), (0,)), ((), ())), preferred_element_type=f32, **kw)


def pack_rows(rows, width):
    heads = rows.shape[0]
    if width >= BLOCK:
        per = width // BLOCK
        lines = [
            jnp.concatenate([rows[i * per + j : i * per + j + 1] for j in range(per)], axis=1)
            for i in range(heads // per)
        ]
    else:
        lines = [rows[:, i * width : (i + 1) * width] for i in range(BLOCK // width)]
    spare = EXTRA - sum(line.shape[0] for line in lines)
    return jnp.concatenate(lines + [jnp.zeros((spare, width), rows.dtype)], axis=0)


def unpack_rows(lines, heads, width):
    if width >= BLOCK:
        per = width // BLOCK
        rows = [
            lines[i : i + 1, j * BLOCK : (j + 1) * BLOCK]
            for i in range(heads // per)
            for j in range(per)
        ]
    else:
        rows = [jnp.concatenate([lines[i : i + 1] for i in range(BLOCK // width)], axis=1)]
    return jnp.concatenate(rows + [jnp.zeros((ROWS - heads, BLOCK), lines.dtype)], axis=0)


def prep_kernel(saved_ref, switch_ref, final_ref, scale_ref, x_ref, dt_ref, out_ref, gate_ref):
    _, _, width = out_ref.shape
    cols = INNER // NORM_GROUPS
    heads = width // HEAD_DIM
    dt_rows = dt_ref[...].astype(f32)
    for n in range(saved_ref.shape[1] // cols):
        at = slice(n * cols, (n + 1) * cols)
        values = saved_ref[:, at].astype(f32)
        switch = switch_ref[:, at].astype(f32)
        cot = final_ref[:, at].astype(f32) * scale_ref[:, at]
        sig = 1.0 / (1.0 + jnp.exp(-switch))
        silu = switch * sig
        g = values * silu
        inv = lax.rsqrt(jnp.mean(g * g, axis=-1, keepdims=True) + EPSILON)
        scaled = g * inv
        d_g = inv * (cot - scaled * jnp.mean(cot * scaled, axis=-1, keepdims=True))
        d_y = (d_g * silu).astype(bf16)
        gate_ref[:, at] = (d_g * values * (sig * (1.0 + switch * (1.0 - sig)))).astype(bf16)
        for c in range(cols // width):
            i = n * (cols // width) + c
            out_ref[i, :BLOCK, :] = x_ref[:, i * width : (i + 1) * width]
            out_ref[i, BLOCK : 2 * BLOCK, :] = d_y[:, c * width : (c + 1) * width]
            out_ref[i, 2 * BLOCK :, :] = pack_rows(
                dt_rows[i * heads : (i + 1) * heads], width
            ).astype(bf16)


def proj_kernel(at_ref, act_ref, *refs):
    count = len(refs) - 2
    own_ref, other_ref = refs[count:]
    size = act_ref.shape[1] // count
    total = jnp.zeros((act_ref.shape[0], refs[0].shape[1]), f32)
    for k in range(count):
        start = pl.multiple_of((at_ref[0] ^ k) * size, size)
        total = total + nn(act_ref[:, pl.ds(start, size)], refs[k][...])
    wide = total.shape[1] // GROUPS
    low = total[:, :wide].astype(bf16)
    high = total[:, wide:].astype(bf16)
    is_low = jnp.broadcast_to(at_ref[2], low.shape) == 0
    own_ref[...] = jnp.where(is_low, low, high)
    other_ref[...] = jnp.where(is_low, high, low)


def hidden_kernel(at_ref, own_ref, other_ref, *refs):
    count = len(refs) - 1
    out_ref = refs[count]
    size = out_ref.shape[1] // count
    own = own_ref[...]
    other = other_ref[...]
    is_low = jnp.broadcast_to(at_ref[2], own.shape) == 0
    both = jnp.concatenate(
        [jnp.where(is_low, own, other), jnp.where(is_low, other, own)], axis=1
    )
    for k in range(count):
        start = pl.multiple_of((at_ref[0] ^ k) * size, size)
        out_ref[:, pl.ds(start, size)] = nt(both, refs[k][...]).astype(bf16)


def weight_kernel(dp, at_ref, *refs):
    grad_refs = refs[:dp]
    act_refs = refs[dp : 2 * dp]
    far_ref, last_ref = refs[2 * dp : 2 * dp + 2]
    out_refs = refs[2 * dp + 2 : -1]
    total_ref = refs[-1]
    total = None
    for k in range(dp):
        for part in range(2):
            far = last_ref[...] if k == dp - 1 else far_ref[k]
            acts = act_refs[k][...] if part == 0 else far
            term = tn(acts, grad_refs[k][part])
            total = term if total is None else total + term
    total_ref[...] = total
    size = out_refs[0].shape[0]
    for k, out_ref in enumerate(out_refs):
        start = pl.multiple_of((at_ref[3] ^ k) * size, size)
        out_ref[...] = total_ref[pl.ds(start, size), :].astype(bf16)


def spread_kernel(half, at_ref, *refs):
    outs = refs[2 * half :]
    size = refs[0].shape[0]
    for part in range(2):
        group = at_ref[2] if part == 0 else 1 - at_ref[2]
        lanes = pl.ds(pl.multiple_of(group * STATE, STATE), STATE)
        for k in range(half):
            rows = pl.ds(pl.multiple_of((at_ref[3] ^ k) * size, size), size)
            chunk = refs[part * half + k][...].astype(f32)
            outs[0][rows, lanes] = chunk[:, :STATE]
            outs[1][rows, lanes] = chunk[:, STATE:]


def gather_kernel(at_ref, *refs):
    for k, ref in enumerate(refs[:-1]):
        refs[-1][k] = ref[...]


def unpack_kernel(back_ref, dx_ref, dt_ref):
    devices, _, width = back_ref.shape
    heads = width // HEAD_DIM
    rows = []
    for i in range(devices):
        dx_ref[:, i * width : (i + 1) * width] = back_ref[i, :BLOCK, :]
        rows.append(unpack_rows(back_ref[i, BLOCK:, :].astype(f32), heads, width)[:heads])
    dt_ref[...] = jnp.concatenate(rows, axis=0).astype(bf16)


def split(value, count):
    terms = []
    for _ in range(count):
        terms.append(value.astype(bf16))
        value = value - terms[-1].astype(f32)
    return terms


def per_head(ref, index):
    total = jnp.zeros(index.shape, f32)
    for h in range(ref.shape[0]):
        total = jnp.where(index == h, ref[h], total)
    return total


def triangle(include):
    r = lax.broadcasted_iota(jnp.int32, (BLOCK, BLOCK), 0)
    c = lax.broadcasted_iota(jnp.int32, (BLOCK, BLOCK), 1)
    return jnp.where(include(r, c), 1.0, 0.0).astype(bf16)


def expand(count, width):
    shape = (count * ROWS, width)
    r = lax.broadcasted_iota(jnp.int32, shape, 0) % ROWS
    c = lax.broadcasted_iota(jnp.int32, shape, 1) // HEAD_DIM
    return jnp.where(r == c, 1.0, 0.0)


PAD = 8


def conv(pad_ref, b, w_ref, flip):
    win = pad_ref[pl.ds(pl.multiple_of(b * BLOCK, BLOCK), BLOCK + 2 * PAD), :]
    total = None
    for k in range(CONV_K):
        shift = (CONV_K - 1) // 2 - k
        moved = win if shift == 0 else pltpu.roll(win, shift % (BLOCK + 2 * PAD), 0)
        tap = w_ref[CONV_K - 1 - k : CONV_K - k, :] if flip else w_ref[k : k + 1, :]
        term = moved[PAD : PAD + BLOCK] * tap
        total = term if total is None else total + term
    return total


def enter_kernel(
    offset_ref,
    fading_ref,
    x_ref,
    drop_ref,
    xw_ref,
    u_ref,
    us_ref,
    row_ref,
    wide_ref,
    dr_ref,
    gg_ref,
    xpad,
):
    blocks, _, width = x_ref.shape
    heads = width // HEAD_DIM
    all_rows = blocks * ROWS
    rows_of = lax.broadcasted_iota(jnp.int32, (ROWS, BLOCK), 0)
    offset = per_head(offset_ref, rows_of)
    fade = jnp.exp(per_head(fading_ref, rows_of))
    xpad[0:PAD, :] = jnp.zeros((PAD, width), f32)
    xpad[PAD + blocks * BLOCK :, :] = jnp.zeros((PAD, width), f32)

    def load_block(b, _):
        at = pl.multiple_of(b * BLOCK, BLOCK) + PAD
        xpad[pl.ds(at, BLOCK), :] = x_ref[b, :BLOCK, :].astype(f32)
        lines = x_ref[b, 2 * BLOCK :, :].astype(f32)
        row_ref[0, b] = unpack_rows(lines, heads, width) + offset
        drop = drop_ref[:, pl.ds(pl.multiple_of(b * BLOCK, BLOCK), BLOCK)]
        row_ref[1, b] = jnp.concatenate([drop, jnp.zeros((ROWS - heads, BLOCK), f32)], axis=0)
        return 0

    lax.fori_loop(0, blocks, load_block, 0)
    raw = row_ref[0].reshape(all_rows, BLOCK)
    dt = jnp.maximum(raw, 0.0) + jnp.log1p(jnp.exp(-jnp.abs(raw)))
    rate = (dt.reshape(blocks, ROWS, BLOCK) * fade[None] + row_ref[1]).reshape(all_rows, BLOCK)
    sums = nn(jnp.concatenate(split(rate, 3), axis=0), triangle(lambda r, c: r <= c))
    cum = sums[:all_rows] + sums[all_rows : 2 * all_rows] + sums[2 * all_rows :]
    total = cum[:, BLOCK - 1 :]
    row_ref[0] = dt.reshape(blocks, ROWS, BLOCK)
    row_ref[1] = cum.reshape(blocks, ROWS, BLOCK)
    row_ref[2] = jnp.exp(-cum).reshape(blocks, ROWS, BLOCK)
    row_ref[3] = jnp.exp(cum - total).reshape(blocks, ROWS, BLOCK)
    row_ref[4] = (1.0 / (1.0 + jnp.exp(-raw))).reshape(blocks, ROWS, BLOCK)

    def body(b, _):
        pre = conv(xpad, b, xw_ref, False)
        sig = 1.0 / (1.0 + jnp.exp(-pre))
        u = pre * sig
        u_ref[b] = u
        us_ref[b] = sig * (1.0 + pre * (1.0 - sig))
        rows = jnp.concatenate([row_ref[0, b], row_ref[2, b], row_ref[3, b]], axis=1)
        wide = tn(jnp.concatenate(split(rows, 3), axis=0), expand(3, width).astype(bf16))
        wide_ref[b] = wide
        w_in = wide[BLOCK : 2 * BLOCK]
        w_out = wide[2 * BLOCK :]
        driven = u * wide[:BLOCK]
        g = x_ref[b, BLOCK : 2 * BLOCK, :].astype(f32)
        dr_ref[b] = jnp.concatenate([driven * w_out, driven * w_in], axis=1).astype(bf16)
        gg_ref[b] = jnp.concatenate([g * w_in, g * w_out], axis=1).astype(bf16)
        return 0

    lax.fori_loop(0, blocks, body, 0, unroll=2)


def mixer_kernel(
    devices,
    at_ref,
    fading_ref,
    direct_ref,
    *refs,
):
    x_ref, u_s, us_s, rows_in, wide_s, dr_s, gg_s, xw_ref, write_ref, read_ref = refs[:10]
    bc_refs = refs[10 : 10 + devices]
    refs = refs[10 + devices :]
    out_ref = refs[0]
    dbc_refs = refs[1 : 1 + devices // 2]
    xpad, bcpad, kcs_s, kr_s, row_s, st_s, car_s, sel_s, bcw_ref = refs[1 + devices // 2 :]
    blocks, _, width = x_ref.shape
    heads = width // HEAD_DIM
    pad = PAD
    lanes = min(width, BLOCK)
    per = lanes // HEAD_DIM
    all_rows = blocks * ROWS
    fade = jnp.exp(per_head(fading_ref, lax.broadcasted_iota(jnp.int32, (ROWS, BLOCK), 0)))

    mine = pl.ds(pl.multiple_of(at_ref[2] * STATE, STATE), STATE)
    bcw_ref[:CONV_K, :STATE] = write_ref[:, mine]
    bcw_ref[:CONV_K, STATE:] = read_ref[:, mine]

    r = lax.broadcasted_iota(jnp.int32, (5 * width, BLOCK), 0)
    c = lax.broadcasted_iota(jnp.int32, (5 * width, BLOCK), 1)
    base = jnp.where(r < 2 * width, 0, jnp.where(r < 4 * width, ROWS, 2 * ROWS))
    sel_s[...] = jnp.where(c == base + (r % width) // HEAD_DIM, 1.0, 0.0).astype(bf16)

    xpad[0:pad, :] = jnp.zeros((pad, width), f32)
    xpad[pad + blocks * BLOCK :, :] = jnp.zeros((pad, width), f32)
    bcpad[0:pad, :] = jnp.zeros((pad, 2 * STATE), f32)
    bcpad[pad + blocks * BLOCK :, :] = jnp.zeros((pad, 2 * STATE), f32)
    for k, bc_ref in enumerate(bc_refs):
        at = pl.multiple_of((at_ref[1] ^ k) * BLOCK, BLOCK) + pad
        bcpad[pl.ds(at, BLOCK), :] = bc_ref[...].astype(f32)

    def first(b, _):
        pre = conv(bcpad, b, bcw_ref, False)
        sig = 1.0 / (1.0 + jnp.exp(-pre))
        act = (pre * sig).astype(bf16)
        kcs_s[b] = sig * (1.0 + pre * (1.0 - sig))
        kr_s[b] = act
        st_s[b, :, : 2 * width] = tn(act[:, :STATE], dr_s[b])
        st_s[b, :, 2 * width :] = tn(act[:, STATE:], gg_s[b])
        return 0

    lax.fori_loop(0, blocks, first, 0, unroll=2)

    def scan(slot, back):
        def step(i, carry):
            b = blocks - 1 - i if back else i
            at = slice(slot * width, (slot + 1) * width)
            car_s[b, :, at] = carry.astype(bf16)
            decay = wide_s[b][2 * BLOCK - 1 : 2 * BLOCK]
            return carry * decay + st_s[b, :, at]

        lax.fori_loop(0, blocks, step, jnp.zeros((STATE, width), f32))

    scan(0, False)
    scan(1, True)
    scan(2, True)
    scan(3, False)

    def second(b, _):
        act = kr_s[b]
        keys = act[:, :STATE]
        reads = act[:, STATE:]
        u = u_s[b]
        g16 = x_ref[b, BLOCK : 2 * BLOCK, :]
        cum = rows_in[1, b]
        cum_t = cum.T
        wide = wide_s[b]
        w_dt = wide[:BLOCK]
        w_in = wide[BLOCK : 2 * BLOCK]
        w_out = wide[2 * BLOCK :]
        driven = (u * w_dt).astype(bf16)
        d_io = dr_s[b]
        g_io = gg_s[b]
        carry = car_s[b]
        c_s = carry[:, : 2 * width]
        c_g = carry[:, 2 * width :]
        y = nn(reads, c_s)
        c = nn(keys, c_g)
        d_r = nt(g_io, c_s)
        d_k = nt(d_io, c_g)
        scores = nt(keys, reads)
        upper = lax.broadcasted_iota(jnp.int32, (BLOCK, BLOCK), 0) > lax.broadcasted_iota(
            jnp.int32, (BLOCK, BLOCK), 1
        )
        lane = lax.broadcasted_iota(jnp.int32, (BLOCK, lanes), 1) // HEAD_DIM
        column = lax.broadcasted_iota(jnp.int32, (BLOCK, BLOCK), 1)
        row = lax.broadcasted_iota(jnp.int32, (ROWS, BLOCK), 0)
        d_scores = None
        d_driven = []
        by_key = jnp.zeros((BLOCK, BLOCK), f32)
        by_read = jnp.zeros((ROWS, BLOCK), f32)
        none = jnp.zeros((BLOCK, lanes), bf16)
        for p in range(width // lanes):
            at = slice(p * lanes, (p + 1) * lanes)
            g_p = g16[:, at]
            d_p = driven[:, at]
            gu = nt(
                jnp.concatenate([jnp.where(lane == j, d_p, none) for j in range(per)], axis=0), g_p
            )
            s_p = []
            for j in range(per):
                h = p * per + j
                decay = jnp.exp(-jnp.abs(cum_t[:, h : h + 1] - cum[h : h + 1, :]))
                gu_h = gu[j * BLOCK : (j + 1) * BLOCK]
                s = scores * decay
                term = gu_h * decay
                d_scores = term if d_scores is None else d_scores + term
                z = s * gu_h
                z = jnp.where(upper, z, -z)
                by_key = jnp.where(column == h, jnp.sum(z, axis=1, keepdims=True), by_key)
                by_read = jnp.where(row == h, jnp.sum(z, axis=0, keepdims=True), by_read)
                s_p.append(s.astype(bf16))
            d_driven.append(
                nn(
                    jnp.concatenate(s_p, axis=1),
                    jnp.concatenate([jnp.where(lane == j, g_p, none) for j in range(per)], axis=0),
                )
            )
        ds16 = d_scores.astype(bf16)
        d_k = d_k + nn(ds16, reads)
        d_r = d_r + tn(ds16, keys)
        c_x = c[:, :width]
        c_y = c[:, width:]
        d_dr = jnp.concatenate(d_driven, axis=1) + w_out * c_x + w_in * c_y
        prefix = d_io[:, :width].astype(f32) * c_x + g_io[:, width:].astype(f32) * y[:, width:]
        suffix = g_io[:, :width].astype(f32) * y[:, :width] + d_io[:, width:].astype(f32) * c_y
        sums = nn(
            jnp.concatenate(
                split(suffix - prefix, 2) + split(prefix, 2) + [(d_dr * u).astype(bf16)], axis=1
            ),
            sel_s[...],
        )
        sums = sums.T
        by_key = by_key.T
        through = jnp.sum(c_s.astype(f32) * c_g.astype(f32), axis=0, keepdims=True)
        through = (through[:, :width] + through[:, width:]) * wide[2 * BLOCK - 1 : 2 * BLOCK]
        through = jnp.sum(expand(1, width) * through, axis=1, keepdims=True)
        before = jnp.sum(sums[ROWS : 2 * ROWS], axis=1, keepdims=True) + through
        row_s[0, b] = sums[:ROWS] + by_key[:ROWS] - by_read
        row_s[1, b] = jnp.broadcast_to(before, (ROWS, BLOCK))
        row_s[2, b] = sums[2 * ROWS : 3 * ROWS]
        skip = per_head(direct_ref, lax.broadcasted_iota(jnp.int32, (1, width), 1) // HEAD_DIM)
        d_u = d_dr * w_dt + g16.astype(f32) * skip
        at = pl.multiple_of(b * BLOCK, BLOCK) + pad
        xpad[pl.ds(at, BLOCK), :] = d_u * us_s[b]
        bcpad[pl.ds(at, BLOCK), :] = jnp.concatenate([d_k, d_r], axis=1) * kcs_s[b]
        return 0

    lax.fori_loop(0, blocks, second, 0, unroll=2)

    sums = nn(
        jnp.concatenate(split(row_s[0].reshape(all_rows, BLOCK), 3), axis=0),
        triangle(lambda r, c: r >= c),
    )
    sums = sums[:all_rows] + sums[all_rows : 2 * all_rows] + sums[2 * all_rows :]
    d_rate = -(sums.reshape(blocks, ROWS, BLOCK) + row_s[1])
    row_s[0] = (row_s[2] + d_rate * fade[None]) * rows_in[4]

    for k, dbc_ref in enumerate(dbc_refs):
        for part in range(2):
            b = at_ref[1] ^ k if part == 0 else at_ref[1] ^ k ^ len(dbc_refs)
            dbc_ref[part] = conv(bcpad, b, bcw_ref, True).astype(bf16)

    def last(b, _):
        out_ref[b, :BLOCK, :] = conv(xpad, b, xw_ref, True).astype(bf16)
        out_ref[b, BLOCK:, :] = pack_rows(row_s[0, b][:heads], width).astype(bf16)
        return 0

    lax.fori_loop(0, blocks, last, 0)


def limit(mib):
    return pltpu.CompilerParams(vmem_limit_bytes=mib << 20)


def vmem():
    return pl.BlockSpec(memory_space=pltpu.VMEM)


def smem():
    return pl.BlockSpec(memory_space=pltpu.SMEM)


def run_enter(offset, fading, x, drop, xw):
    blocks, _, width = x.shape
    shape = jax.ShapeDtypeStruct
    return pl.pallas_call(
        enter_kernel,
        out_shape=(
            shape((blocks, BLOCK, width), f32),
            shape((blocks, BLOCK, width), f32),
            shape((5, blocks, ROWS, BLOCK), f32),
            shape((blocks, 3 * BLOCK, width), f32),
            shape((blocks, BLOCK, 2 * width), bf16),
            shape((blocks, BLOCK, 2 * width), bf16),
        ),
        in_specs=[smem()] * 2 + [vmem()] * 3,
        out_specs=(vmem(),) * 6,
        scratch_shapes=[pltpu.VMEM((blocks * BLOCK + 2 * PAD, width), f32)],
        compiler_params=limit(24),
        name="enter",
    )(offset, fading, x, drop, xw)


def run_mixer(at, fading, direct, x, entered, filters, bc):
    blocks, _, width = x.shape
    length = blocks * BLOCK
    scratch = [
        pltpu.VMEM((length + 2 * PAD, width), f32),
        pltpu.VMEM((length + 2 * PAD, 2 * STATE), f32),
        pltpu.VMEM((blocks, BLOCK, 2 * STATE), f32),
        pltpu.VMEM((blocks, BLOCK, 2 * STATE), bf16),
        pltpu.VMEM((3, blocks, ROWS, BLOCK), f32),
        pltpu.VMEM((blocks, STATE, 4 * width), f32),
        pltpu.VMEM((blocks, STATE, 4 * width), bf16),
        pltpu.VMEM((5 * width, BLOCK), bf16),
        pltpu.VMEM((ROWS, 2 * STATE), f32),
    ]
    half = len(bc) // 2
    outs = pl.pallas_call(
        functools.partial(mixer_kernel, len(bc)),
        out_shape=(jax.ShapeDtypeStruct((blocks, BLOCK + EXTRA, width), bf16),)
        + (jax.ShapeDtypeStruct((2, BLOCK, 2 * STATE), bf16),) * half,
        in_specs=[smem()] * 3 + [vmem()] * (10 + len(bc)),
        out_specs=(vmem(),) * (1 + half),
        scratch_shapes=scratch,
        compiler_params=limit(36),
        name="mixer",
    )(at, fading, direct, x, *entered, *filters, *bc)
    return outs[0], outs[1:]


def swap(value, axis, bits):
    size = lax.axis_size(axis)
    return lax.ppermute(value, axis, [(i, i ^ bits) for i in range(size)])


def call(kernel, outs, *args, scratch=()):
    specs = [smem()] + [vmem()] * (len(args) - 1)
    return pl.pallas_call(
        kernel,
        out_shape=outs,
        in_specs=specs,
        out_specs=jax.tree.map(lambda _: vmem(), outs),
        scratch_shapes=scratch,
        compiler_params=limit(16),
    )(*args)


def local(
    layer_activity,
    writer_matrix,
    reader_matrix,
    source_unfiltered,
    switch_raw_signal,
    saved_result,
    final_adjoint,
    delta_raw,
    extra_logdrop,
    source_filter_coefs,
    writer_filter_coefs,
    reader_filter_coefs,
    delta_offset,
    fading_exponents,
    direct_factor,
    rescale_factor,
):
    tokens = layer_activity.shape[1]
    width_in = layer_activity.shape[2]
    dp = lax.axis_size("dp")
    sp = lax.axis_size("sp")
    half = sp // 2
    heads = delta_offset.shape[0]
    width = heads * HEAD_DIM
    me_d = lax.axis_index("dp")
    me_s = lax.axis_index("sp")
    at = jnp.stack([me_d, me_s, me_s // half, me_s % half]).astype(jnp.int32)
    shape = jax.ShapeDtypeStruct
    rows = layer_activity[0]
    share = width_in // dp

    weights = jnp.concatenate(
        [
            m[:, g * STATE : (g + 1) * STATE]
            for g in range(GROUPS)
            for m in (writer_matrix, reader_matrix)
        ],
        axis=1,
    )
    pieces = {0: weights}
    bit = dp // 2
    while bit:
        moved = {k ^ bit: swap(v, "dp", bit) for k, v in list(pieces.items())}
        pieces.update(moved)
        bit //= 2
    pieces = [pieces[k] for k in range(dp)]

    steps = NORM_GROUPS // 2
    wide = INNER // steps
    row_spec = pl.BlockSpec((tokens, wide), lambda i: (0, i))
    packed, d_gate = pl.pallas_call(
        prep_kernel,
        grid=(steps,),
        in_specs=[
            row_spec,
            row_spec,
            row_spec,
            pl.BlockSpec((1, wide), lambda i: (0, i)),
            row_spec,
            pl.BlockSpec((HEADS // steps, tokens), lambda i: (i, 0)),
        ],
        out_specs=(
            pl.BlockSpec((sp // steps, 2 * BLOCK + EXTRA, width), lambda i: (i, 0, 0)),
            row_spec,
        ),
        out_shape=(
            shape((sp, 2 * BLOCK + EXTRA, width), bf16),
            shape((tokens, INNER), bf16),
        ),
        name="prep",
    )(
        saved_result[0],
        switch_raw_signal[0],
        final_adjoint[0],
        rescale_factor[None],
        source_unfiltered[0],
        delta_raw[0].T,
    )
    heads_x = lax.all_to_all(packed, "sp", 0, 0, tiled=True)

    acts = [lax.dynamic_slice(rows, (0, (me_d ^ k) * share), (tokens, share)) for k in range(dp)]
    acts = [acts[0]] + [swap(acts[k], "dp", k) for k in range(1, dp)]
    gathered = call(gather_kernel, shape((dp - 1, tokens, share), bf16), at, *acts[: dp - 1])
    acts += [swap(gathered, "sp", half), swap(acts[dp - 1], "sp", half)]

    bc = shape((tokens, 2 * STATE), bf16)
    own, other = call(proj_kernel, (bc, bc), at, rows, *pieces)
    other = swap(other, "sp", half)
    all_bc = [own if k == 0 else swap(own, "sp", k) for k in range(half)]
    all_bc += [other if k == 0 else swap(other, "sp", k) for k in range(half)]

    entered = run_enter(
        delta_offset, fading_exponents, heads_x, extra_logdrop[0].T, source_filter_coefs
    )
    filters = (source_filter_coefs, writer_filter_coefs, reader_filter_coefs)
    d_x, d_bc = run_mixer(at, fading_exponents, direct_factor, heads_x, entered, filters, all_bc)

    parts = [d_bc[0]] + [swap(d_bc[k], "sp", k) for k in range(1, half)]
    grads = functools.reduce(jnp.add, [p.astype(f32) for p in parts]).astype(bf16)
    back_x = lax.all_to_all(d_x, "sp", 0, 0, tiled=True)
    all_grads = [grads if k == 0 else swap(grads, "dp", k) for k in range(dp)]
    rest = swap(grads[1], "sp", half)

    chunk = shape((share // half, 2 * STATE), bf16)
    chunks = call(
        functools.partial(weight_kernel, dp),
        (chunk,) * half,
        at,
        *all_grads,
        *acts,
        scratch=[pltpu.VMEM((share, 2 * STATE), f32)],
    )
    chunks = [chunks[0]] + [swap(chunks[k], "sp", k) for k in range(1, half)]
    mine = functools.reduce(jnp.add, [c.astype(f32) for c in chunks]).astype(bf16)
    theirs = swap(mine, "sp", half)
    placed = [mine if k == 0 else swap(mine, "sp", k) for k in range(half)]
    placed += [theirs if k == 0 else swap(theirs, "sp", k) for k in range(half)]

    d_hidden = call(hidden_kernel, shape((tokens, width_in), bf16), at, grads[0], rest, *pieces)
    d_source, d_delta = pl.pallas_call(
        unpack_kernel,
        out_shape=(shape((tokens, INNER), bf16), shape((HEADS, tokens), bf16)),
        in_specs=[vmem()],
        out_specs=(vmem(), vmem()),
        compiler_params=limit(16),
        name="unpack",
    )(back_x)
    matrix = shape((share, GROUPS * STATE), f32)
    d_w_b, d_w_c = call(functools.partial(spread_kernel, half), (matrix, matrix), at, *placed)
    return d_hidden[None], d_source[None], d_gate[None], d_delta.T[None], d_w_b, d_w_c


def solution(mesh):
    in_specs = (
        P("dp", "sp", None),
        P("dp", None),
        P("dp", None),
        P("dp", "sp", None),
        P("dp", "sp", None),
        P("dp", "sp", None),
        P("dp", "sp", None),
        P("dp", "sp", None),
        P("dp", None, "sp"),
        P(None, "sp"),
        P(),
        P(),
        P("sp"),
        P("sp"),
        P("sp"),
        P(),
    )
    out_specs = (
        P("dp", "sp", None),
        P("dp", "sp", None),
        P("dp", "sp", None),
        P("dp", "sp", None),
        P("dp", None),
        P("dp", None),
    )

    return jax.shard_map(local, mesh=mesh, in_specs=in_specs, out_specs=out_specs, check_vma=False)
```

```python
import functools

import jax
import jax.numpy as jnp
from jax import lax
from jax.experimental import pallas as pl
from jax.experimental.pallas import tpu as pltpu
from jax.sharding import PartitionSpec as P


HEADS = 32
HEAD_DIM = 64
STATE = 128
GROUPS = 2
NORM_GROUPS = 8
CONV_K = 5
BLOCK = 128
INNER = 2048
EXTRA = 8
ROWS = 8

EPSILON = 1e-06
f32 = jnp.float32
bf16 = jnp.bfloat16


def nn(a, b, **kw):
    return lax.dot_general(a, b, (((1,), (0,)), ((), ())), preferred_element_type=f32, **kw)


def nt(a, b, **kw):
    return lax.dot_general(a, b, (((1,), (1,)), ((), ())), preferred_element_type=f32, **kw)


def tn(a, b, **kw):
    return lax.dot_general(a, b, (((0,), (0,)), ((), ())), preferred_element_type=f32, **kw)


def pack_rows(rows, width):
    heads = rows.shape[0]
    if width >= BLOCK:
        per = width // BLOCK
        lines = [
            jnp.concatenate([rows[i * per + j : i * per + j + 1] for j in range(per)], axis=1)
            for i in range(heads // per)
        ]
    else:
        lines = [rows[:, i * width : (i + 1) * width] for i in range(BLOCK // width)]
    spare = EXTRA - sum(line.shape[0] for line in lines)
    return jnp.concatenate(lines + [jnp.zeros((spare, width), rows.dtype)], axis=0)


def unpack_rows(lines, heads, width):
    if width >= BLOCK:
        per = width // BLOCK
        rows = [
            lines[i : i + 1, j * BLOCK : (j + 1) * BLOCK]
            for i in range(heads // per)
            for j in range(per)
        ]
    else:
        rows = [jnp.concatenate([lines[i : i + 1] for i in range(BLOCK // width)], axis=1)]
    return jnp.concatenate(rows + [jnp.zeros((ROWS - heads, BLOCK), lines.dtype)], axis=0)


def prep_kernel(saved_ref, switch_ref, final_ref, scale_ref, x_ref, dt_ref, out_ref, gate_ref):
    _, _, width = out_ref.shape
    cols = INNER // NORM_GROUPS
    heads = width // HEAD_DIM
    dt_rows = dt_ref[...].astype(f32)
    for n in range(saved_ref.shape[1] // cols):
        at = slice(n * cols, (n + 1) * cols)
        values = saved_ref[:, at].astype(f32)
        switch = switch_ref[:, at].astype(f32)
        cot = final_ref[:, at].astype(f32) * scale_ref[:, at]
        sig = 1.0 / (1.0 + jnp.exp(-switch))
        silu = switch * sig
        g = values * silu
        inv = lax.rsqrt(jnp.mean(g * g, axis=-1, keepdims=True) + EPSILON)
        scaled = g * inv
        d_g = inv * (cot - scaled * jnp.mean(cot * scaled, axis=-1, keepdims=True))
        d_y = (d_g * silu).astype(bf16)
        gate_ref[:, at] = (d_g * values * (sig * (1.0 + switch * (1.0 - sig)))).astype(bf16)
        for c in range(cols // width):
            i = n * (cols // width) + c
            out_ref[i, :BLOCK, :] = x_ref[:, i * width : (i + 1) * width]
            out_ref[i, BLOCK : 2 * BLOCK, :] = d_y[:, c * width : (c + 1) * width]
            out_ref[i, 2 * BLOCK :, :] = pack_rows(
                dt_rows[i * heads : (i + 1) * heads], width
            ).astype(bf16)


def proj_kernel(at_ref, act_ref, *refs):
    count = len(refs) - 2
    own_ref, other_ref = refs[count:]
    size = act_ref.shape[1] // count
    total = jnp.zeros((act_ref.shape[0], refs[0].shape[1]), f32)
    for k in range(count):
        start = pl.multiple_of((at_ref[0] ^ k) * size, size)
        total = total + nn(act_ref[:, pl.ds(start, size)], refs[k][...])
    wide = total.shape[1] // GROUPS
    low = total[:, :wide].astype(bf16)
    high = total[:, wide:].astype(bf16)
    is_low = jnp.broadcast_to(at_ref[2], low.shape) == 0
    own_ref[...] = jnp.where(is_low, low, high)
    other_ref[...] = jnp.where(is_low, high, low)


def hidden_kernel(at_ref, own_ref, other_ref, *refs):
    count = len(refs) - 1
    out_ref = refs[count]
    size = out_ref.shape[1] // count
    own = own_ref[...]
    other = other_ref[...]
    is_low = jnp.broadcast_to(at_ref[2], own.shape) == 0
    both = jnp.concatenate(
        [jnp.where(is_low, own, other), jnp.where(is_low, other, own)], axis=1
    )
    for k in range(count):
        start = pl.multiple_of((at_ref[0] ^ k) * size, size)
        out_ref[:, pl.ds(start, size)] = nt(both, refs[k][...]).astype(bf16)


def weight_kernel(dp, at_ref, *refs):
    grad_refs = refs[:dp]
    act_refs = refs[dp : 2 * dp]
    far_ref, last_ref = refs[2 * dp : 2 * dp + 2]
    out_refs = refs[2 * dp + 2 : -1]
    total_ref = refs[-1]
    total = None
    for k in range(dp):
        for part in range(2):
            far = last_ref[...] if k == dp - 1 else far_ref[k]
            acts = act_refs[k][...] if part == 0 else far
            term = tn(acts, grad_refs[k][part])
            total = term if total is None else total + term
    total_ref[...] = total
    size = out_refs[0].shape[0]
    for k, out_ref in enumerate(out_refs):
        start = pl.multiple_of((at_ref[3] ^ k) * size, size)
        out_ref[...] = total_ref[pl.ds(start, size), :].astype(bf16)


def spread_kernel(half, at_ref, *refs):
    outs = refs[2 * half :]
    size = refs[0].shape[0]
    for part in range(2):
        group = at_ref[2] if part == 0 else 1 - at_ref[2]
        lanes = pl.ds(pl.multiple_of(group * STATE, STATE), STATE)
        for k in range(half):
            rows = pl.ds(pl.multiple_of((at_ref[3] ^ k) * size, size), size)
            chunk = refs[part * half + k][...].astype(f32)
            outs[0][rows, lanes] = chunk[:, :STATE]
            outs[1][rows, lanes] = chunk[:, STATE:]


def gather_kernel(at_ref, drop_ref, *refs):
    for k, ref in enumerate(refs[:-2]):
        refs[-2][k] = ref[...]
    refs[-1][...] = drop_ref[...]


def unpack_kernel(back_ref, dx_ref, dt_ref):
    devices, _, width = back_ref.shape
    heads = width // HEAD_DIM
    rows = []
    for i in range(devices):
        dx_ref[:, i * width : (i + 1) * width] = back_ref[i, :BLOCK, :]
        rows.append(unpack_rows(back_ref[i, BLOCK:, :].astype(f32), heads, width)[:heads])
    dt_ref[...] = jnp.concatenate(rows, axis=0).astype(bf16)


def split(value, count):
    terms = []
    for _ in range(count):
        terms.append(value.astype(bf16))
        value = value - terms[-1].astype(f32)
    return terms


def per_head(ref, line, index):
    total = jnp.zeros(index.shape, f32)
    for h in range(ref.shape[1]):
        total = jnp.where(index == h, ref[line, h], total)
    return total


def triangle(include):
    r = lax.broadcasted_iota(jnp.int32, (BLOCK, BLOCK), 0)
    c = lax.broadcasted_iota(jnp.int32, (BLOCK, BLOCK), 1)
    return jnp.where(include(r, c), 1.0, 0.0).astype(bf16)


def expand(count, width):
    shape = (count * ROWS, width)
    r = lax.broadcasted_iota(jnp.int32, shape, 0) % ROWS
    c = lax.broadcasted_iota(jnp.int32, shape, 1) // HEAD_DIM
    return jnp.where(r == c, 1.0, 0.0)


PAD = 8


def conv(pad_ref, b, w_ref, flip):
    win = pad_ref[pl.ds(pl.multiple_of(b * BLOCK, BLOCK), BLOCK + 2 * PAD), :]
    total = None
    for k in range(CONV_K):
        shift = (CONV_K - 1) // 2 - k
        moved = win if shift == 0 else pltpu.roll(win, shift % (BLOCK + 2 * PAD), 0)
        tap = w_ref[CONV_K - 1 - k : CONV_K - k, :] if flip else w_ref[k : k + 1, :]
        term = moved[PAD : PAD + BLOCK] * tap
        total = term if total is None else total + term
    return total


def enter_kernel(
    head_ref,
    x_ref,
    drop_ref,
    xw_ref,
    u_ref,
    us_ref,
    row_ref,
    wide_ref,
    dr_ref,
    gg_ref,
    xpad,
):
    blocks, _, width = x_ref.shape
    heads = width // HEAD_DIM
    all_rows = blocks * ROWS
    rows_of = lax.broadcasted_iota(jnp.int32, (ROWS, BLOCK), 0)
    offset = per_head(head_ref, 0, rows_of)
    fade = jnp.exp(per_head(head_ref, 1, rows_of))
    xpad[0:PAD, :] = jnp.zeros((PAD, width), f32)
    xpad[PAD + blocks * BLOCK :, :] = jnp.zeros((PAD, width), f32)

    def load_block(b, _):
        at = pl.multiple_of(b * BLOCK, BLOCK) + PAD
        xpad[pl.ds(at, BLOCK), :] = x_ref[b, :BLOCK, :].astype(f32)
        lines = x_ref[b, 2 * BLOCK :, :].astype(f32)
        row_ref[0, b] = unpack_rows(lines, heads, width) + offset
        drop = drop_ref[:, pl.ds(pl.multiple_of(b * BLOCK, BLOCK), BLOCK)]
        row_ref[1, b] = jnp.concatenate([drop, jnp.zeros((ROWS - heads, BLOCK), f32)], axis=0)
        return 0

    lax.fori_loop(0, blocks, load_block, 0)
    raw = row_ref[0].reshape(all_rows, BLOCK)
    dt = jnp.maximum(raw, 0.0) + jnp.log1p(jnp.exp(-jnp.abs(raw)))
    rate = (dt.reshape(blocks, ROWS, BLOCK) * fade[None] + row_ref[1]).reshape(all_rows, BLOCK)
    sums = nn(jnp.concatenate(split(rate, 3), axis=0), triangle(lambda r, c: r <= c))
    cum = sums[:all_rows] + sums[all_rows : 2 * all_rows] + sums[2 * all_rows :]
    total = cum[:, BLOCK - 1 :]
    row_ref[0] = dt.reshape(blocks, ROWS, BLOCK)
    row_ref[1] = cum.reshape(blocks, ROWS, BLOCK)
    row_ref[2] = jnp.exp(-cum).reshape(blocks, ROWS, BLOCK)
    row_ref[3] = jnp.exp(cum - total).reshape(blocks, ROWS, BLOCK)
    row_ref[4] = (1.0 / (1.0 + jnp.exp(-raw))).reshape(blocks, ROWS, BLOCK)

    def body(b, _):
        pre = conv(xpad, b, xw_ref, False)
        sig = 1.0 / (1.0 + jnp.exp(-pre))
        u = pre * sig
        u_ref[b] = u
        us_ref[b] = sig * (1.0 + pre * (1.0 - sig))
        rows = jnp.concatenate([row_ref[0, b], row_ref[2, b], row_ref[3, b]], axis=1)
        wide = tn(jnp.concatenate(split(rows, 3), axis=0), expand(3, width).astype(bf16))
        wide_ref[b] = wide
        w_in = wide[BLOCK : 2 * BLOCK]
        w_out = wide[2 * BLOCK :]
        driven = u * wide[:BLOCK]
        g = x_ref[b, BLOCK : 2 * BLOCK, :].astype(f32)
        dr_ref[b] = jnp.concatenate([driven * w_out, driven * w_in], axis=1).astype(bf16)
        gg_ref[b] = jnp.concatenate([g * w_in, g * w_out], axis=1).astype(bf16)
        return 0

    lax.fori_loop(0, blocks, body, 0, unroll=2)


def mixer_kernel(
    devices,
    at_ref,
    head_ref,
    *refs,
):
    x_ref, u_s, us_s, rows_in, wide_s, dr_s, gg_s, xw_ref, write_ref, read_ref = refs[:10]
    bc_refs = refs[10 : 10 + devices]
    refs = refs[10 + devices :]
    out_ref = refs[0]
    dbc_refs = refs[1 : 1 + devices // 2]
    xpad, bcpad, kcs_s, kr_s, row_s, st_s, car_s, sel_s, bcw_ref, stage, sems = refs[
        1 + devices // 2 :
    ]
    copies = [
        pltpu.make_async_copy(bc_ref, stage.at[k], sems.at[k]) for k, bc_ref in enumerate(bc_refs)
    ]
    for copy in copies:
        copy.start()
    blocks, _, width = x_ref.shape
    heads = width // HEAD_DIM
    pad = PAD
    lanes = min(width, BLOCK)
    per = lanes // HEAD_DIM
    all_rows = blocks * ROWS
    fade = jnp.exp(per_head(head_ref, 1, lax.broadcasted_iota(jnp.int32, (ROWS, BLOCK), 0)))

    mine = pl.ds(pl.multiple_of(at_ref[2] * STATE, STATE), STATE)
    bcw_ref[:CONV_K, :STATE] = write_ref[:, mine]
    bcw_ref[:CONV_K, STATE:] = read_ref[:, mine]

    r = lax.broadcasted_iota(jnp.int32, (5 * width, BLOCK), 0)
    c = lax.broadcasted_iota(jnp.int32, (5 * width, BLOCK), 1)
    base = jnp.where(r < 2 * width, 0, jnp.where(r < 4 * width, ROWS, 2 * ROWS))
    sel_s[...] = jnp.where(c == base + (r % width) // HEAD_DIM, 1.0, 0.0).astype(bf16)

    xpad[0:pad, :] = jnp.zeros((pad, width), f32)
    xpad[pad + blocks * BLOCK :, :] = jnp.zeros((pad, width), f32)
    bcpad[0:pad, :] = jnp.zeros((pad, 2 * STATE), f32)
    bcpad[pad + blocks * BLOCK :, :] = jnp.zeros((pad, 2 * STATE), f32)
    for k, copy in enumerate(copies):
        copy.wait()
        at = pl.multiple_of((at_ref[1] ^ k) * BLOCK, BLOCK) + pad
        bcpad[pl.ds(at, BLOCK), :] = stage[k].astype(f32)

    def first(b, _):
        pre = conv(bcpad, b, bcw_ref, False)
        sig = 1.0 / (1.0 + jnp.exp(-pre))
        act = (pre * sig).astype(bf16)
        kcs_s[b] = sig * (1.0 + pre * (1.0 - sig))
        kr_s[b] = act
        st_s[b, :, : 2 * width] = tn(act[:, :STATE], dr_s[b])
        st_s[b, :, 2 * width :] = tn(act[:, STATE:], gg_s[b])
        return 0

    lax.fori_loop(0, blocks, first, 0, unroll=2)

    def scan(slot, back):
        def step(i, carry):
            b = blocks - 1 - i if back else i
            at = slice(slot * width, (slot + 1) * width)
            car_s[b, :, at] = carry.astype(bf16)
            decay = wide_s[b][2 * BLOCK - 1 : 2 * BLOCK]
            return carry * decay + st_s[b, :, at]

        lax.fori_loop(0, blocks, step, jnp.zeros((STATE, width), f32))

    scan(0, False)
    scan(1, True)
    scan(2, True)
    scan(3, False)

    def second(b, _):
        act = kr_s[b]
        keys = act[:, :STATE]
        reads = act[:, STATE:]
        u = u_s[b]
        g16 = x_ref[b, BLOCK : 2 * BLOCK, :]
        cum = rows_in[1, b]
        cum_t = cum.T
        wide = wide_s[b]
        w_dt = wide[:BLOCK]
        w_in = wide[BLOCK : 2 * BLOCK]
        w_out = wide[2 * BLOCK :]
        driven = (u * w_dt).astype(bf16)
        d_io = dr_s[b]
        g_io = gg_s[b]
        carry = car_s[b]
        c_s = carry[:, : 2 * width]
        c_g = carry[:, 2 * width :]
        y = nn(reads, c_s)
        c = nn(keys, c_g)
        d_r = nt(g_io, c_s)
        d_k = nt(d_io, c_g)
        scores = nt(keys, reads)
        upper = lax.broadcasted_iota(jnp.int32, (BLOCK, BLOCK), 0) > lax.broadcasted_iota(
            jnp.int32, (BLOCK, BLOCK), 1
        )
        lane = lax.broadcasted_iota(jnp.int32, (BLOCK, lanes), 1) // HEAD_DIM
        column = lax.broadcasted_iota(jnp.int32, (BLOCK, BLOCK), 1)
        row = lax.broadcasted_iota(jnp.int32, (ROWS, BLOCK), 0)
        d_scores = None
        d_driven = []
        by_key = jnp.zeros((BLOCK, BLOCK), f32)
        by_read = jnp.zeros((ROWS, BLOCK), f32)
        none = jnp.zeros((BLOCK, lanes), bf16)
        for p in range(width // lanes):
            at = slice(p * lanes, (p + 1) * lanes)
            g_p = g16[:, at]
            d_p = driven[:, at]
            gu = nt(
                jnp.concatenate([jnp.where(lane == j, d_p, none) for j in range(per)], axis=0), g_p
            )
            s_p = []
            for j in range(per):
                h = p * per + j
                decay = jnp.exp(-jnp.abs(cum_t[:, h : h + 1] - cum[h : h + 1, :]))
                gu_h = gu[j * BLOCK : (j + 1) * BLOCK]
                s = scores * decay
                term = gu_h * decay
                d_scores = term if d_scores is None else d_scores + term
                z = s * gu_h
                z = jnp.where(upper, z, -z)
                by_key = jnp.where(column == h, jnp.sum(z, axis=1, keepdims=True), by_key)
                by_read = jnp.where(row == h, jnp.sum(z, axis=0, keepdims=True), by_read)
                s_p.append(s.astype(bf16))
            d_driven.append(
                nn(
                    jnp.concatenate(s_p, axis=1),
                    jnp.concatenate([jnp.where(lane == j, g_p, none) for j in range(per)], axis=0),
                )
            )
        ds16 = d_scores.astype(bf16)
        d_k = d_k + nn(ds16, reads)
        d_r = d_r + tn(ds16, keys)
        c_x = c[:, :width]
        c_y = c[:, width:]
        d_dr = jnp.concatenate(d_driven, axis=1) + w_out * c_x + w_in * c_y
        prefix = d_io[:, :width].astype(f32) * c_x + g_io[:, width:].astype(f32) * y[:, width:]
        suffix = g_io[:, :width].astype(f32) * y[:, :width] + d_io[:, width:].astype(f32) * c_y
        sums = nn(
            jnp.concatenate(
                split(suffix - prefix, 2) + split(prefix, 2) + [(d_dr * u).astype(bf16)], axis=1
            ),
            sel_s[...],
        )
        sums = sums.T
        by_key = by_key.T
        through = jnp.sum(c_s.astype(f32) * c_g.astype(f32), axis=0, keepdims=True)
        through = (through[:, :width] + through[:, width:]) * wide[2 * BLOCK - 1 : 2 * BLOCK]
        through = jnp.sum(expand(1, width) * through, axis=1, keepdims=True)
        before = jnp.sum(sums[ROWS : 2 * ROWS], axis=1, keepdims=True) + through
        row_s[0, b] = sums[:ROWS] + by_key[:ROWS] - by_read
        row_s[1, b] = jnp.broadcast_to(before, (ROWS, BLOCK))
        row_s[2, b] = sums[2 * ROWS : 3 * ROWS]
        skip = per_head(head_ref, 2, lax.broadcasted_iota(jnp.int32, (1, width), 1) // HEAD_DIM)
        d_u = d_dr * w_dt + g16.astype(f32) * skip
        at = pl.multiple_of(b * BLOCK, BLOCK) + pad
        xpad[pl.ds(at, BLOCK), :] = d_u * us_s[b]
        bcpad[pl.ds(at, BLOCK), :] = jnp.concatenate([d_k, d_r], axis=1) * kcs_s[b]
        return 0

    lax.fori_loop(0, blocks, second, 0, unroll=2)

    sums = nn(
        jnp.concatenate(split(row_s[0].reshape(all_rows, BLOCK), 3), axis=0),
        triangle(lambda r, c: r >= c),
    )
    sums = sums[:all_rows] + sums[all_rows : 2 * all_rows] + sums[2 * all_rows :]
    d_rate = -(sums.reshape(blocks, ROWS, BLOCK) + row_s[1])
    row_s[0] = (row_s[2] + d_rate * fade[None]) * rows_in[4]

    for k, dbc_ref in enumerate(dbc_refs):
        for part in range(2):
            b = at_ref[1] ^ k if part == 0 else at_ref[1] ^ k ^ len(dbc_refs)
            dbc_ref[part] = conv(bcpad, b, bcw_ref, True).astype(bf16)

    def last(b, _):
        out_ref[b, :BLOCK, :] = conv(xpad, b, xw_ref, True).astype(bf16)
        out_ref[b, BLOCK:, :] = pack_rows(row_s[0, b][:heads], width).astype(bf16)
        return 0

    lax.fori_loop(0, blocks, last, 0)


def limit(mib):
    return pltpu.CompilerParams(vmem_limit_bytes=mib << 20)


def vmem():
    return pl.BlockSpec(memory_space=pltpu.VMEM)


def smem():
    return pl.BlockSpec(memory_space=pltpu.SMEM)


def run_enter(per_heads, x, drop, xw):
    blocks, _, width = x.shape
    shape = jax.ShapeDtypeStruct
    return pl.pallas_call(
        enter_kernel,
        out_shape=(
            shape((blocks, BLOCK, width), f32),
            shape((blocks, BLOCK, width), f32),
            shape((5, blocks, ROWS, BLOCK), f32),
            shape((blocks, 3 * BLOCK, width), f32),
            shape((blocks, BLOCK, 2 * width), bf16),
            shape((blocks, BLOCK, 2 * width), bf16),
        ),
        in_specs=[smem()] + [vmem()] * 3,
        out_specs=(vmem(),) * 6,
        scratch_shapes=[pltpu.VMEM((blocks * BLOCK + 2 * PAD, width), f32)],
        compiler_params=limit(min(60, 12 * max(1, blocks // 8))),
        name="enter",
    )(per_heads, x, drop, xw)


def run_mixer(at, per_heads, x, entered, filters, bc):
    blocks, _, width = x.shape
    length = blocks * BLOCK
    scratch = [
        pltpu.VMEM((length + 2 * PAD, width), f32),
        pltpu.VMEM((length + 2 * PAD, 2 * STATE), f32),
        pltpu.VMEM((blocks, BLOCK, 2 * STATE), f32),
        pltpu.VMEM((blocks, BLOCK, 2 * STATE), bf16),
        pltpu.VMEM((3, blocks, ROWS, BLOCK), f32),
        pltpu.VMEM((blocks, STATE, 4 * width), f32),
        pltpu.VMEM((blocks, STATE, 4 * width), bf16),
        pltpu.VMEM((5 * width, BLOCK), bf16),
        pltpu.VMEM((ROWS, 2 * STATE), f32),
        pltpu.VMEM((len(bc), BLOCK, 2 * STATE), bf16),
        pltpu.SemaphoreType.DMA((len(bc),)),
    ]
    half = len(bc) // 2
    outs = pl.pallas_call(
        functools.partial(mixer_kernel, len(bc)),
        out_shape=(jax.ShapeDtypeStruct((blocks, BLOCK + EXTRA, width), bf16),)
        + (jax.ShapeDtypeStruct((2, BLOCK, 2 * STATE), bf16),) * half,
        in_specs=[smem()] * 2
        + [vmem()] * 10
        + [pl.BlockSpec(memory_space=pltpu.HBM)] * len(bc),
        out_specs=(vmem(),) * (1 + half),
        scratch_shapes=scratch,
        compiler_params=limit(min(60, 20 * max(1, blocks // 8))),
        name="mixer",
    )(at, per_heads, x, *entered, *filters, *bc)
    return outs[0], outs[1:]


def swap(value, axis, bits):
    size = lax.axis_size(axis)
    return lax.ppermute(value, axis, [(i, i ^ bits) for i in range(size)])


def call(kernel, outs, *args, scratch=()):
    specs = [smem()] + [vmem()] * (len(args) - 1)
    return pl.pallas_call(
        kernel,
        out_shape=outs,
        in_specs=specs,
        out_specs=jax.tree.map(lambda _: vmem(), outs),
        scratch_shapes=scratch,
        compiler_params=limit(8),
    )(*args)


def local(
    layer_activity,
    writer_matrix,
    reader_matrix,
    source_unfiltered,
    switch_raw_signal,
    saved_result,
    final_adjoint,
    delta_raw,
    extra_logdrop,
    source_filter_coefs,
    writer_filter_coefs,
    reader_filter_coefs,
    delta_offset,
    fading_exponents,
    direct_factor,
    rescale_factor,
):
    tokens = layer_activity.shape[1]
    width_in = layer_activity.shape[2]
    dp = lax.axis_size("dp")
    sp = lax.axis_size("sp")
    half = sp // 2
    heads = delta_offset.shape[0]
    width = heads * HEAD_DIM
    me_d = lax.axis_index("dp")
    me_s = lax.axis_index("sp")
    at = jnp.stack([me_d, me_s, me_s // half, me_s % half]).astype(jnp.int32)
    shape = jax.ShapeDtypeStruct
    rows = layer_activity[0]
    share = width_in // dp

    weights = jnp.concatenate(
        [
            m[:, g * STATE : (g + 1) * STATE]
            for g in range(GROUPS)
            for m in (writer_matrix, reader_matrix)
        ],
        axis=1,
    )
    pieces = {0: weights}
    bit = dp // 2
    while bit:
        moved = {k ^ bit: swap(v, "dp", bit) for k, v in list(pieces.items())}
        pieces.update(moved)
        bit //= 2
    pieces = [pieces[k] for k in range(dp)]

    steps = NORM_GROUPS // 2
    wide = INNER // steps
    row_spec = pl.BlockSpec((tokens, wide), lambda i: (0, i))
    packed, d_gate = pl.pallas_call(
        prep_kernel,
        grid=(steps,),
        in_specs=[
            row_spec,
            row_spec,
            row_spec,
            pl.BlockSpec((1, wide), lambda i: (0, i)),
            row_spec,
            pl.BlockSpec((HEADS // steps, tokens), lambda i: (i, 0)),
        ],
        out_specs=(
            pl.BlockSpec((sp // steps, 2 * BLOCK + EXTRA, width), lambda i: (i, 0, 0)),
            row_spec,
        ),
        out_shape=(
            shape((sp, 2 * BLOCK + EXTRA, width), bf16),
            shape((tokens, INNER), bf16),
        ),
        name="prep",
    )(
        saved_result[0],
        switch_raw_signal[0],
        final_adjoint[0],
        rescale_factor[None],
        source_unfiltered[0],
        delta_raw[0].T,
    )
    heads_x = lax.all_to_all(packed, "sp", 0, 0, tiled=True)

    acts = [lax.dynamic_slice(rows, (0, (me_d ^ k) * share), (tokens, share)) for k in range(dp)]
    acts = [acts[0]] + [swap(acts[k], "dp", k) for k in range(1, dp)]
    drop = extra_logdrop[0].T
    gathered, drop = call(
        gather_kernel,
        (shape((dp - 1, tokens, share), bf16), shape(drop.shape, f32)),
        at,
        drop,
        *acts[: dp - 1],
    )
    acts += [swap(gathered, "sp", half), swap(acts[dp - 1], "sp", half)]

    bc = shape((tokens, 2 * STATE), bf16)
    own, other = call(proj_kernel, (bc, bc), at, rows, *pieces)
    other = swap(other, "sp", half)
    all_bc = [own if k == 0 else swap(own, "sp", k) for k in range(half)]
    all_bc += [other if k == 0 else swap(other, "sp", k) for k in range(half)]

    per_heads = jnp.stack([delta_offset, fading_exponents, direct_factor])
    entered = run_enter(per_heads, heads_x, drop, source_filter_coefs)
    filters = (source_filter_coefs, writer_filter_coefs, reader_filter_coefs)
    d_x, d_bc = run_mixer(at, per_heads, heads_x, entered, filters, all_bc)

    parts = [d_bc[0]] + [swap(d_bc[k], "sp", k) for k in range(1, half)]
    grads = functools.reduce(jnp.add, [p.astype(f32) for p in parts]).astype(bf16)
    back_x = lax.all_to_all(d_x, "sp", 0, 0, tiled=True)
    all_grads = [grads if k == 0 else swap(grads, "dp", k) for k in range(dp)]
    rest = swap(grads[1], "sp", half)

    chunk = shape((share // half, 2 * STATE), bf16)
    chunks = call(
        functools.partial(weight_kernel, dp),
        (chunk,) * half,
        at,
        *all_grads,
        *acts,
        scratch=[pltpu.VMEM((share, 2 * STATE), f32)],
    )
    chunks = [chunks[0]] + [swap(chunks[k], "sp", k) for k in range(1, half)]
    mine = functools.reduce(jnp.add, [c.astype(f32) for c in chunks]).astype(bf16)
    theirs = swap(mine, "sp", half)
    placed = [mine if k == 0 else swap(mine, "sp", k) for k in range(half)]
    placed += [theirs if k == 0 else swap(theirs, "sp", k) for k in range(half)]

    d_hidden = call(hidden_kernel, shape((tokens, width_in), bf16), at, grads[0], rest, *pieces)
    d_source, d_delta = pl.pallas_call(
        unpack_kernel,
        out_shape=(shape((tokens, INNER), bf16), shape((HEADS, tokens), bf16)),
        in_specs=[vmem()],
        out_specs=(vmem(), vmem()),
        compiler_params=limit(8),
        name="unpack",
    )(back_x)
    matrix = shape((share, GROUPS * STATE), f32)
    d_w_b, d_w_c = call(functools.partial(spread_kernel, half), (matrix, matrix), at, *placed)
    return d_hidden[None], d_source[None], d_gate[None], d_delta.T[None], d_w_b, d_w_c


def solution(mesh):
    in_specs = (
        P("dp", "sp", None),
        P("dp", None),
        P("dp", None),
        P("dp", "sp", None),
        P("dp", "sp", None),
        P("dp", "sp", None),
        P("dp", "sp", None),
        P("dp", "sp", None),
        P("dp", None, "sp"),
        P(None, "sp"),
        P(),
        P(),
        P("sp"),
        P("sp"),
        P("sp"),
        P(),
    )
    out_specs = (
        P("dp", "sp", None),
        P("dp", "sp", None),
        P("dp", "sp", None),
        P("dp", "sp", None),
        P("dp", None),
        P("dp", None),
    )

    return jax.shard_map(local, mesh=mesh, in_specs=in_specs, out_specs=out_specs, check_vma=False)
```

```python
import functools

import jax
import jax.numpy as jnp
from jax import lax
from jax.experimental import pallas as pl
from jax.experimental.pallas import tpu as pltpu
from jax.sharding import PartitionSpec as P


HEADS = 32
HEAD_DIM = 64
STATE = 128
GROUPS = 2
NORM_GROUPS = 8
CONV_K = 5
BLOCK = 128
INNER = 2048
EXTRA = 8
ROWS = 8

EPSILON = 1e-06
f32 = jnp.float32
bf16 = jnp.bfloat16


def nn(a, b, **kw):
    return lax.dot_general(a, b, (((1,), (0,)), ((), ())), preferred_element_type=f32, **kw)


def nt(a, b, **kw):
    return lax.dot_general(a, b, (((1,), (1,)), ((), ())), preferred_element_type=f32, **kw)


def tn(a, b, **kw):
    return lax.dot_general(a, b, (((0,), (0,)), ((), ())), preferred_element_type=f32, **kw)


def pack_rows(rows, width):
    heads = rows.shape[0]
    if width >= BLOCK:
        per = width // BLOCK
        lines = [
            jnp.concatenate([rows[i * per + j : i * per + j + 1] for j in range(per)], axis=1)
            for i in range(heads // per)
        ]
    else:
        lines = [rows[:, i * width : (i + 1) * width] for i in range(BLOCK // width)]
    spare = EXTRA - sum(line.shape[0] for line in lines)
    return jnp.concatenate(lines + [jnp.zeros((spare, width), rows.dtype)], axis=0)


def unpack_rows(lines, heads, width):
    if width >= BLOCK:
        per = width // BLOCK
        rows = [
            lines[i : i + 1, j * BLOCK : (j + 1) * BLOCK]
            for i in range(heads // per)
            for j in range(per)
        ]
    else:
        rows = [jnp.concatenate([lines[i : i + 1] for i in range(BLOCK // width)], axis=1)]
    return jnp.concatenate(rows + [jnp.zeros((ROWS - heads, BLOCK), lines.dtype)], axis=0)


def prep_kernel(saved_ref, switch_ref, final_ref, scale_ref, x_ref, dt_ref, out_ref, gate_ref):
    _, _, width = out_ref.shape
    cols = INNER // NORM_GROUPS
    heads = width // HEAD_DIM
    dt_rows = dt_ref[...].astype(f32)
    for n in range(saved_ref.shape[1] // cols):
        at = slice(n * cols, (n + 1) * cols)
        values = saved_ref[:, at].astype(f32)
        switch = switch_ref[:, at].astype(f32)
        cot = final_ref[:, at].astype(f32) * scale_ref[:, at]
        sig = 1.0 / (1.0 + jnp.exp(-switch))
        silu = switch * sig
        g = values * silu
        inv = lax.rsqrt(jnp.mean(g * g, axis=-1, keepdims=True) + EPSILON)
        scaled = g * inv
        d_g = inv * (cot - scaled * jnp.mean(cot * scaled, axis=-1, keepdims=True))
        d_y = (d_g * silu).astype(bf16)
        gate_ref[:, at] = (d_g * values * (sig * (1.0 + switch * (1.0 - sig)))).astype(bf16)
        for c in range(cols // width):
            i = n * (cols // width) + c
            out_ref[i, :BLOCK, :] = x_ref[:, i * width : (i + 1) * width]
            out_ref[i, BLOCK : 2 * BLOCK, :] = d_y[:, c * width : (c + 1) * width]
            out_ref[i, 2 * BLOCK :, :] = pack_rows(
                dt_rows[i * heads : (i + 1) * heads], width
            ).astype(bf16)


def proj_kernel(at_ref, act_ref, *refs):
    count = len(refs) - 2
    own_ref, other_ref = refs[count:]
    size = act_ref.shape[1] // count
    total = jnp.zeros((act_ref.shape[0], refs[0].shape[1]), f32)
    for k in range(count):
        start = pl.multiple_of((at_ref[0] ^ k) * size, size)
        total = total + nn(act_ref[:, pl.ds(start, size)], refs[k][...])
    wide = total.shape[1] // GROUPS
    low = total[:, :wide].astype(bf16)
    high = total[:, wide:].astype(bf16)
    is_low = jnp.broadcast_to(at_ref[2], low.shape) == 0
    own_ref[...] = jnp.where(is_low, low, high)
    other_ref[...] = jnp.where(is_low, high, low)


def hidden_kernel(at_ref, own_ref, other_ref, *refs):
    count = len(refs) - 1
    out_ref = refs[count]
    size = out_ref.shape[1] // count
    own = own_ref[...]
    other = other_ref[...]
    is_low = jnp.broadcast_to(at_ref[2], own.shape) == 0
    both = jnp.concatenate(
        [jnp.where(is_low, own, other), jnp.where(is_low, other, own)], axis=1
    )
    for k in range(count):
        start = pl.multiple_of((at_ref[0] ^ k) * size, size)
        out_ref[:, pl.ds(start, size)] = nt(both, refs[k][...]).astype(bf16)


def weight_kernel(dp, at_ref, *refs):
    grad_refs = refs[:dp]
    act_refs = refs[dp : 2 * dp]
    far_ref, last_ref = refs[2 * dp : 2 * dp + 2]
    out_refs = refs[2 * dp + 2 : -1]
    total_ref = refs[-1]
    total = None
    for k in range(dp):
        for part in range(2):
            far = last_ref[...] if k == dp - 1 else far_ref[k]
            acts = act_refs[k][...] if part == 0 else far
            term = tn(acts, grad_refs[k][part])
            total = term if total is None else total + term
    total_ref[...] = total
    size = out_refs[0].shape[0]
    for k, out_ref in enumerate(out_refs):
        start = pl.multiple_of((at_ref[3] ^ k) * size, size)
        out_ref[...] = total_ref[pl.ds(start, size), :].astype(bf16)


def spread_kernel(half, at_ref, *refs):
    outs = refs[2 * half :]
    size = refs[0].shape[0]
    for part in range(2):
        group = at_ref[2] if part == 0 else 1 - at_ref[2]
        lanes = pl.ds(pl.multiple_of(group * STATE, STATE), STATE)
        for k in range(half):
            rows = pl.ds(pl.multiple_of((at_ref[3] ^ k) * size, size), size)
            chunk = refs[part * half + k][...].astype(f32)
            outs[0][rows, lanes] = chunk[:, :STATE]
            outs[1][rows, lanes] = chunk[:, STATE:]


def gather_kernel(at_ref, drop_ref, *refs):
    for k, ref in enumerate(refs[:-2]):
        refs[-2][k] = ref[...]
    refs[-1][...] = drop_ref[...]


def unpack_kernel(back_ref, dx_ref, dt_ref):
    devices, _, width = back_ref.shape
    heads = width // HEAD_DIM
    rows = []
    for i in range(devices):
        dx_ref[:, i * width : (i + 1) * width] = back_ref[i, :BLOCK, :]
        rows.append(unpack_rows(back_ref[i, BLOCK:, :].astype(f32), heads, width)[:heads])
    dt_ref[...] = jnp.concatenate(rows, axis=0).astype(bf16)


def split(value, count):
    terms = []
    for _ in range(count):
        terms.append(value.astype(bf16))
        value = value - terms[-1].astype(f32)
    return terms


def per_head(ref, line, index):
    total = jnp.zeros(index.shape, f32)
    for h in range(ref.shape[1]):
        total = jnp.where(index == h, ref[line, h], total)
    return total


def triangle(include):
    r = lax.broadcasted_iota(jnp.int32, (BLOCK, BLOCK), 0)
    c = lax.broadcasted_iota(jnp.int32, (BLOCK, BLOCK), 1)
    return jnp.where(include(r, c), 1.0, 0.0).astype(bf16)


def expand(count, width):
    shape = (count * ROWS, width)
    r = lax.broadcasted_iota(jnp.int32, shape, 0) % ROWS
    c = lax.broadcasted_iota(jnp.int32, shape, 1) // HEAD_DIM
    return jnp.where(r == c, 1.0, 0.0)


PAD = 8


def conv(pad_ref, b, w_ref, flip):
    win = pad_ref[pl.ds(pl.multiple_of(b * BLOCK, BLOCK), BLOCK + 2 * PAD), :]
    total = None
    for k in range(CONV_K):
        shift = (CONV_K - 1) // 2 - k
        moved = win if shift == 0 else pltpu.roll(win, shift % (BLOCK + 2 * PAD), 0)
        tap = w_ref[CONV_K - 1 - k : CONV_K - k, :] if flip else w_ref[k : k + 1, :]
        term = moved[PAD : PAD + BLOCK] * tap
        total = term if total is None else total + term
    return total


def enter_kernel(
    head_ref,
    x_ref,
    drop_ref,
    xw_ref,
    u_ref,
    us_ref,
    row_ref,
    wide_ref,
    dr_ref,
    gg_ref,
    xpad,
):
    blocks, _, width = x_ref.shape
    heads = width // HEAD_DIM
    all_rows = blocks * ROWS
    rows_of = lax.broadcasted_iota(jnp.int32, (ROWS, BLOCK), 0)
    offset = per_head(head_ref, 0, rows_of)
    fade = jnp.exp(per_head(head_ref, 1, rows_of))
    xpad[0:PAD, :] = jnp.zeros((PAD, width), f32)
    xpad[PAD + blocks * BLOCK :, :] = jnp.zeros((PAD, width), f32)

    def load_block(b, _):
        at = pl.multiple_of(b * BLOCK, BLOCK) + PAD
        xpad[pl.ds(at, BLOCK), :] = x_ref[b, :BLOCK, :].astype(f32)
        lines = x_ref[b, 2 * BLOCK :, :].astype(f32)
        row_ref[0, b] = unpack_rows(lines, heads, width) + offset
        drop = drop_ref[:, pl.ds(pl.multiple_of(b * BLOCK, BLOCK), BLOCK)]
        row_ref[1, b] = jnp.concatenate([drop, jnp.zeros((ROWS - heads, BLOCK), f32)], axis=0)
        return 0

    lax.fori_loop(0, blocks, load_block, 0)
    raw = row_ref[0].reshape(all_rows, BLOCK)
    dt = jnp.maximum(raw, 0.0) + jnp.log1p(jnp.exp(-jnp.abs(raw)))
    rate = (dt.reshape(blocks, ROWS, BLOCK) * fade[None] + row_ref[1]).reshape(all_rows, BLOCK)
    sums = nn(jnp.concatenate(split(rate, 3), axis=0), triangle(lambda r, c: r <= c))
    cum = sums[:all_rows] + sums[all_rows : 2 * all_rows] + sums[2 * all_rows :]
    total = cum[:, BLOCK - 1 :]
    row_ref[0] = dt.reshape(blocks, ROWS, BLOCK)
    row_ref[1] = cum.reshape(blocks, ROWS, BLOCK)
    row_ref[2] = jnp.exp(-cum).reshape(blocks, ROWS, BLOCK)
    row_ref[3] = jnp.exp(cum - total).reshape(blocks, ROWS, BLOCK)
    row_ref[4] = (1.0 / (1.0 + jnp.exp(-raw))).reshape(blocks, ROWS, BLOCK)

    def body(b, _):
        pre = conv(xpad, b, xw_ref, False)
        sig = 1.0 / (1.0 + jnp.exp(-pre))
        u = pre * sig
        u_ref[b] = u
        us_ref[b] = sig * (1.0 + pre * (1.0 - sig))
        rows = jnp.concatenate([row_ref[0, b], row_ref[2, b], row_ref[3, b]], axis=1)
        wide = tn(jnp.concatenate(split(rows, 3), axis=0), expand(3, width).astype(bf16))
        wide_ref[b] = wide
        w_in = wide[BLOCK : 2 * BLOCK]
        w_out = wide[2 * BLOCK :]
        driven = u * wide[:BLOCK]
        g = x_ref[b, BLOCK : 2 * BLOCK, :].astype(f32)
        dr_ref[b] = jnp.concatenate([driven * w_out, driven * w_in], axis=1).astype(bf16)
        gg_ref[b] = jnp.concatenate([g * w_in, g * w_out], axis=1).astype(bf16)
        return 0

    lax.fori_loop(0, blocks, body, 0, unroll=2)


def mixer_kernel(
    devices,
    at_ref,
    head_ref,
    *refs,
):
    x_ref, u_s, us_s, rows_in, wide_s, dr_s, gg_s, xw_ref, write_ref, read_ref = refs[:10]
    bc_refs = refs[10 : 10 + devices]
    refs = refs[10 + devices :]
    out_ref = refs[0]
    dbc_refs = refs[1 : 1 + devices // 2]
    xpad, bcpad, kcs_s, kr_s, row_s, st_s, car_s, sel_s, bcw_ref, stage, sems = refs[
        1 + devices // 2 :
    ]
    copies = [
        pltpu.make_async_copy(bc_ref, stage.at[k], sems.at[k]) for k, bc_ref in enumerate(bc_refs)
    ]
    for copy in copies:
        copy.start()
    blocks, _, width = x_ref.shape
    heads = width // HEAD_DIM
    pad = PAD
    lanes = min(width, BLOCK)
    per = lanes // HEAD_DIM
    all_rows = blocks * ROWS
    fade = jnp.exp(per_head(head_ref, 1, lax.broadcasted_iota(jnp.int32, (ROWS, BLOCK), 0)))

    mine = pl.ds(pl.multiple_of(at_ref[2] * STATE, STATE), STATE)
    bcw_ref[:CONV_K, :STATE] = write_ref[:, mine]
    bcw_ref[:CONV_K, STATE:] = read_ref[:, mine]

    r = lax.broadcasted_iota(jnp.int32, (5 * width, BLOCK), 0)
    c = lax.broadcasted_iota(jnp.int32, (5 * width, BLOCK), 1)
    base = jnp.where(r < 2 * width, 0, jnp.where(r < 4 * width, ROWS, 2 * ROWS))
    sel_s[...] = jnp.where(c == base + (r % width) // HEAD_DIM, 1.0, 0.0).astype(bf16)

    xpad[0:pad, :] = jnp.zeros((pad, width), f32)
    xpad[pad + blocks * BLOCK :, :] = jnp.zeros((pad, width), f32)
    bcpad[0:pad, :] = jnp.zeros((pad, 2 * STATE), f32)
    bcpad[pad + blocks * BLOCK :, :] = jnp.zeros((pad, 2 * STATE), f32)
    for k, copy in enumerate(copies):
        copy.wait()
        at = pl.multiple_of((at_ref[1] ^ k) * BLOCK, BLOCK) + pad
        bcpad[pl.ds(at, BLOCK), :] = stage[k].astype(f32)

    def first(b, _):
        pre = conv(bcpad, b, bcw_ref, False)
        sig = 1.0 / (1.0 + jnp.exp(-pre))
        act = (pre * sig).astype(bf16)
        kcs_s[b] = sig * (1.0 + pre * (1.0 - sig))
        kr_s[b] = act
        st_s[b, :, : 2 * width] = tn(act[:, :STATE], dr_s[b])
        st_s[b, :, 2 * width :] = tn(act[:, STATE:], gg_s[b])
        return 0

    lax.fori_loop(0, blocks, first, 0, unroll=2)

    def scan(slot, back):
        def step(i, carry):
            b = blocks - 1 - i if back else i
            at = slice(slot * width, (slot + 1) * width)
            car_s[b, :, at] = carry.astype(bf16)
            decay = wide_s[b][2 * BLOCK - 1 : 2 * BLOCK]
            return carry * decay + st_s[b, :, at]

        lax.fori_loop(0, blocks, step, jnp.zeros((STATE, width), f32))

    scan(0, False)
    scan(1, True)
    scan(2, True)
    scan(3, False)

    def second(b, _):
        act = kr_s[b]
        keys = act[:, :STATE]
        reads = act[:, STATE:]
        u = u_s[b]
        g16 = x_ref[b, BLOCK : 2 * BLOCK, :]
        cum = rows_in[1, b]
        cum_t = cum.T
        wide = wide_s[b]
        w_dt = wide[:BLOCK]
        w_in = wide[BLOCK : 2 * BLOCK]
        w_out = wide[2 * BLOCK :]
        driven = (u * w_dt).astype(bf16)
        d_io = dr_s[b]
        g_io = gg_s[b]
        carry = car_s[b]
        c_s = carry[:, : 2 * width]
        c_g = carry[:, 2 * width :]
        y = nn(reads, c_s)
        c = nn(keys, c_g)
        d_r = nt(g_io, c_s)
        d_k = nt(d_io, c_g)
        scores = nt(keys, reads)
        upper = lax.broadcasted_iota(jnp.int32, (BLOCK, BLOCK), 0) > lax.broadcasted_iota(
            jnp.int32, (BLOCK, BLOCK), 1
        )
        lane = lax.broadcasted_iota(jnp.int32, (BLOCK, lanes), 1) // HEAD_DIM
        column = lax.broadcasted_iota(jnp.int32, (BLOCK, BLOCK), 1)
        row = lax.broadcasted_iota(jnp.int32, (ROWS, BLOCK), 0)
        d_scores = None
        d_driven = []
        by_key = jnp.zeros((BLOCK, BLOCK), f32)
        by_read = jnp.zeros((ROWS, BLOCK), f32)
        none = jnp.zeros((BLOCK, lanes), bf16)
        for p in range(width // lanes):
            at = slice(p * lanes, (p + 1) * lanes)
            g_p = g16[:, at]
            d_p = driven[:, at]
            gu = nt(
                jnp.concatenate([jnp.where(lane == j, d_p, none) for j in range(per)], axis=0), g_p
            )
            s_p = []
            for j in range(per):
                h = p * per + j
                decay = jnp.exp(-jnp.abs(cum_t[:, h : h + 1] - cum[h : h + 1, :]))
                gu_h = gu[j * BLOCK : (j + 1) * BLOCK]
                s = scores * decay
                term = gu_h * decay
                d_scores = term if d_scores is None else d_scores + term
                z = s * gu_h
                z = jnp.where(upper, z, -z)
                by_key = jnp.where(column == h, jnp.sum(z, axis=1, keepdims=True), by_key)
                by_read = jnp.where(row == h, jnp.sum(z, axis=0, keepdims=True), by_read)
                s_p.append(s.astype(bf16))
            d_driven.append(
                nn(
                    jnp.concatenate(s_p, axis=1),
                    jnp.concatenate([jnp.where(lane == j, g_p, none) for j in range(per)], axis=0),
                )
            )
        ds16 = d_scores.astype(bf16)
        d_k = d_k + nn(ds16, reads)
        d_r = d_r + tn(ds16, keys)
        c_x = c[:, :width]
        c_y = c[:, width:]
        d_dr = jnp.concatenate(d_driven, axis=1) + w_out * c_x + w_in * c_y
        prefix = d_io[:, :width].astype(f32) * c_x + g_io[:, width:].astype(f32) * y[:, width:]
        suffix = g_io[:, :width].astype(f32) * y[:, :width] + d_io[:, width:].astype(f32) * c_y
        sums = nn(
            jnp.concatenate(
                split(suffix - prefix, 2) + split(prefix, 2) + [(d_dr * u).astype(bf16)], axis=1
            ),
            sel_s[...],
        )
        sums = sums.T
        by_key = by_key.T
        through = jnp.sum(c_s.astype(f32) * c_g.astype(f32), axis=0, keepdims=True)
        through = (through[:, :width] + through[:, width:]) * wide[2 * BLOCK - 1 : 2 * BLOCK]
        through = jnp.sum(expand(1, width) * through, axis=1, keepdims=True)
        before = jnp.sum(sums[ROWS : 2 * ROWS], axis=1, keepdims=True) + through
        row_s[0, b] = sums[:ROWS] + by_key[:ROWS] - by_read
        row_s[1, b] = jnp.broadcast_to(before, (ROWS, BLOCK))
        row_s[2, b] = sums[2 * ROWS : 3 * ROWS]
        skip = per_head(head_ref, 2, lax.broadcasted_iota(jnp.int32, (1, width), 1) // HEAD_DIM)
        d_u = d_dr * w_dt + g16.astype(f32) * skip
        at = pl.multiple_of(b * BLOCK, BLOCK) + pad
        xpad[pl.ds(at, BLOCK), :] = d_u * us_s[b]
        bcpad[pl.ds(at, BLOCK), :] = jnp.concatenate([d_k, d_r], axis=1) * kcs_s[b]
        return 0

    lax.fori_loop(0, blocks, second, 0, unroll=2)

    sums = nn(
        jnp.concatenate(split(row_s[0].reshape(all_rows, BLOCK), 3), axis=0),
        triangle(lambda r, c: r >= c),
    )
    sums = sums[:all_rows] + sums[all_rows : 2 * all_rows] + sums[2 * all_rows :]
    d_rate = -(sums.reshape(blocks, ROWS, BLOCK) + row_s[1])
    row_s[0] = (row_s[2] + d_rate * fade[None]) * rows_in[4]

    for k, dbc_ref in enumerate(dbc_refs):
        for part in range(2):
            b = at_ref[1] ^ k if part == 0 else at_ref[1] ^ k ^ len(dbc_refs)
            dbc_ref[part] = conv(bcpad, b, bcw_ref, True).astype(bf16)

    def last(b, _):
        out_ref[b, :BLOCK, :] = conv(xpad, b, xw_ref, True).astype(bf16)
        out_ref[b, BLOCK:, :] = pack_rows(row_s[0, b][:heads], width).astype(bf16)
        return 0

    lax.fori_loop(0, blocks, last, 0)


def limit(mib):
    return pltpu.CompilerParams(vmem_limit_bytes=mib << 20)


def vmem():
    return pl.BlockSpec(memory_space=pltpu.VMEM)


def smem():
    return pl.BlockSpec(memory_space=pltpu.SMEM)


def run_enter(per_heads, x, drop, xw):
    blocks, _, width = x.shape
    shape = jax.ShapeDtypeStruct
    return pl.pallas_call(
        enter_kernel,
        out_shape=(
            shape((blocks, BLOCK, width), f32),
            shape((blocks, BLOCK, width), f32),
            shape((5, blocks, ROWS, BLOCK), f32),
            shape((blocks, 3 * BLOCK, width), f32),
            shape((blocks, BLOCK, 2 * width), bf16),
            shape((blocks, BLOCK, 2 * width), bf16),
        ),
        in_specs=[smem()] + [vmem()] * 3,
        out_specs=(vmem(),) * 6,
        scratch_shapes=[pltpu.VMEM((blocks * BLOCK + 2 * PAD, width), f32)],
        compiler_params=limit(min(60, 24 * max(1, blocks // 8))),
        name="enter",
    )(per_heads, x, drop, xw)


def run_mixer(at, per_heads, x, entered, filters, bc):
    blocks, _, width = x.shape
    length = blocks * BLOCK
    scratch = [
        pltpu.VMEM((length + 2 * PAD, width), f32),
        pltpu.VMEM((length + 2 * PAD, 2 * STATE), f32),
        pltpu.VMEM((blocks, BLOCK, 2 * STATE), f32),
        pltpu.VMEM((blocks, BLOCK, 2 * STATE), bf16),
        pltpu.VMEM((3, blocks, ROWS, BLOCK), f32),
        pltpu.VMEM((blocks, STATE, 4 * width), f32),
        pltpu.VMEM((blocks, STATE, 4 * width), bf16),
        pltpu.VMEM((5 * width, BLOCK), bf16),
        pltpu.VMEM((ROWS, 2 * STATE), f32),
        pltpu.VMEM((len(bc), BLOCK, 2 * STATE), bf16),
        pltpu.SemaphoreType.DMA((len(bc),)),
    ]
    half = len(bc) // 2
    outs = pl.pallas_call(
        functools.partial(mixer_kernel, len(bc)),
        out_shape=(jax.ShapeDtypeStruct((blocks, BLOCK + EXTRA, width), bf16),)
        + (jax.ShapeDtypeStruct((2, BLOCK, 2 * STATE), bf16),) * half,
        in_specs=[smem()] * 2
        + [vmem()] * 10
        + [pl.BlockSpec(memory_space=pltpu.HBM)] * len(bc),
        out_specs=(vmem(),) * (1 + half),
        scratch_shapes=scratch,
        compiler_params=limit(min(60, 40 * max(1, blocks // 8))),
        name="mixer",
    )(at, per_heads, x, *entered, *filters, *bc)
    return outs[0], outs[1:]


def swap(value, axis, bits):
    size = lax.axis_size(axis)
    return lax.ppermute(value, axis, [(i, i ^ bits) for i in range(size)])


def call(kernel, outs, *args, scratch=()):
    specs = [smem()] + [vmem()] * (len(args) - 1)
    return pl.pallas_call(
        kernel,
        out_shape=outs,
        in_specs=specs,
        out_specs=jax.tree.map(lambda _: vmem(), outs),
        scratch_shapes=scratch,
        compiler_params=limit(16),
    )(*args)


def local(
    layer_activity,
    writer_matrix,
    reader_matrix,
    source_unfiltered,
    switch_raw_signal,
    saved_result,
    final_adjoint,
    delta_raw,
    extra_logdrop,
    source_filter_coefs,
    writer_filter_coefs,
    reader_filter_coefs,
    delta_offset,
    fading_exponents,
    direct_factor,
    rescale_factor,
):
    tokens = layer_activity.shape[1]
    width_in = layer_activity.shape[2]
    dp = lax.axis_size("dp")
    sp = lax.axis_size("sp")
    half = sp // 2
    heads = delta_offset.shape[0]
    width = heads * HEAD_DIM
    me_d = lax.axis_index("dp")
    me_s = lax.axis_index("sp")
    at = jnp.stack([me_d, me_s, me_s // half, me_s % half]).astype(jnp.int32)
    shape = jax.ShapeDtypeStruct
    rows = layer_activity[0]
    share = width_in // dp

    weights = jnp.concatenate(
        [
            m[:, g * STATE : (g + 1) * STATE]
            for g in range(GROUPS)
            for m in (writer_matrix, reader_matrix)
        ],
        axis=1,
    )
    pieces = {0: weights}
    bit = dp // 2
    while bit:
        moved = {k ^ bit: swap(v, "dp", bit) for k, v in list(pieces.items())}
        pieces.update(moved)
        bit //= 2
    pieces = [pieces[k] for k in range(dp)]

    steps = NORM_GROUPS // 2
    wide = INNER // steps
    row_spec = pl.BlockSpec((tokens, wide), lambda i: (0, i))
    packed, d_gate = pl.pallas_call(
        prep_kernel,
        grid=(steps,),
        in_specs=[
            row_spec,
            row_spec,
            row_spec,
            pl.BlockSpec((1, wide), lambda i: (0, i)),
            row_spec,
            pl.BlockSpec((HEADS // steps, tokens), lambda i: (i, 0)),
        ],
        out_specs=(
            pl.BlockSpec((sp // steps, 2 * BLOCK + EXTRA, width), lambda i: (i, 0, 0)),
            row_spec,
        ),
        out_shape=(
            shape((sp, 2 * BLOCK + EXTRA, width), bf16),
            shape((tokens, INNER), bf16),
        ),
        name="prep",
    )(
        saved_result[0],
        switch_raw_signal[0],
        final_adjoint[0],
        rescale_factor[None],
        source_unfiltered[0],
        delta_raw[0].T,
    )
    heads_x = lax.all_to_all(packed, "sp", 0, 0, tiled=True)

    acts = [lax.dynamic_slice(rows, (0, (me_d ^ k) * share), (tokens, share)) for k in range(dp)]
    acts = [acts[0]] + [swap(acts[k], "dp", k) for k in range(1, dp)]
    drop = extra_logdrop[0].T
    gathered, drop = call(
        gather_kernel,
        (shape((dp - 1, tokens, share), bf16), shape(drop.shape, f32)),
        at,
        drop,
        *acts[: dp - 1],
    )
    acts += [swap(gathered, "sp", half), swap(acts[dp - 1], "sp", half)]

    bc = shape((tokens, 2 * STATE), bf16)
    own, other = call(proj_kernel, (bc, bc), at, rows, *pieces)
    other = swap(other, "sp", half)
    all_bc = [own if k == 0 else swap(own, "sp", k) for k in range(half)]
    all_bc += [other if k == 0 else swap(other, "sp", k) for k in range(half)]

    per_heads = jnp.stack([delta_offset, fading_exponents, direct_factor])
    entered = run_enter(per_heads, heads_x, drop, source_filter_coefs)
    filters = (source_filter_coefs, writer_filter_coefs, reader_filter_coefs)
    d_x, d_bc = run_mixer(at, per_heads, heads_x, entered, filters, all_bc)

    parts = [d_bc[0]] + [swap(d_bc[k], "sp", k) for k in range(1, half)]
    grads = functools.reduce(jnp.add, [p.astype(f32) for p in parts]).astype(bf16)
    back_x = lax.all_to_all(d_x, "sp", 0, 0, tiled=True)
    all_grads = [grads if k == 0 else swap(grads, "dp", k) for k in range(dp)]
    rest = swap(grads[1], "sp", half)

    chunk = shape((share // half, 2 * STATE), bf16)
    chunks = call(
        functools.partial(weight_kernel, dp),
        (chunk,) * half,
        at,
        *all_grads,
        *acts,
        scratch=[pltpu.VMEM((share, 2 * STATE), f32)],
    )
    chunks = [chunks[0]] + [swap(chunks[k], "sp", k) for k in range(1, half)]
    mine = functools.reduce(jnp.add, [c.astype(f32) for c in chunks]).astype(bf16)
    theirs = swap(mine, "sp", half)
    placed = [mine if k == 0 else swap(mine, "sp", k) for k in range(half)]
    placed += [theirs if k == 0 else swap(theirs, "sp", k) for k in range(half)]

    d_hidden = call(hidden_kernel, shape((tokens, width_in), bf16), at, grads[0], rest, *pieces)
    d_source, d_delta = pl.pallas_call(
        unpack_kernel,
        out_shape=(shape((tokens, INNER), bf16), shape((HEADS, tokens), bf16)),
        in_specs=[vmem()],
        out_specs=(vmem(), vmem()),
        compiler_params=limit(16),
        name="unpack",
    )(back_x)
    matrix = shape((share, GROUPS * STATE), f32)
    d_w_b, d_w_c = call(functools.partial(spread_kernel, half), (matrix, matrix), at, *placed)
    return d_hidden[None], d_source[None], d_gate[None], d_delta.T[None], d_w_b, d_w_c


def solution(mesh):
    in_specs = (
        P("dp", "sp", None),
        P("dp", None),
        P("dp", None),
        P("dp", "sp", None),
        P("dp", "sp", None),
        P("dp", "sp", None),
        P("dp", "sp", None),
        P("dp", "sp", None),
        P("dp", None, "sp"),
        P(None, "sp"),
        P(),
        P(),
        P("sp"),
        P("sp"),
        P("sp"),
        P(),
    )
    out_specs = (
        P("dp", "sp", None),
        P("dp", "sp", None),
        P("dp", "sp", None),
        P("dp", "sp", None),
        P("dp", None),
        P("dp", None),
    )

    return jax.shard_map(local, mesh=mesh, in_specs=in_specs, out_specs=out_specs, check_vma=False)
```

```python
import functools

import jax
import jax.numpy as jnp
from jax import lax
from jax.experimental import pallas as pl
from jax.experimental.pallas import tpu as pltpu
from jax.sharding import PartitionSpec as P


HEADS = 32
HEAD_DIM = 64
STATE = 128
GROUPS = 2
NORM_GROUPS = 8
CONV_K = 5
BLOCK = 128
INNER = 2048
EXTRA = 8
ROWS = 8

EPSILON = 1e-06
f32 = jnp.float32
bf16 = jnp.bfloat16


def nn(a, b, **kw):
    return lax.dot_general(a, b, (((1,), (0,)), ((), ())), preferred_element_type=f32, **kw)


def nt(a, b, **kw):
    return lax.dot_general(a, b, (((1,), (1,)), ((), ())), preferred_element_type=f32, **kw)


def tn(a, b, **kw):
    return lax.dot_general(a, b, (((0,), (0,)), ((), ())), preferred_element_type=f32, **kw)


def pack_rows(rows, width):
    heads = rows.shape[0]
    if width >= BLOCK:
        per = width // BLOCK
        lines = [
            jnp.concatenate([rows[i * per + j : i * per + j + 1] for j in range(per)], axis=1)
            for i in range(heads // per)
        ]
    else:
        lines = [rows[:, i * width : (i + 1) * width] for i in range(BLOCK // width)]
    spare = EXTRA - sum(line.shape[0] for line in lines)
    return jnp.concatenate(lines + [jnp.zeros((spare, width), rows.dtype)], axis=0)


def unpack_rows(lines, heads, width):
    if width >= BLOCK:
        per = width // BLOCK
        rows = [
            lines[i : i + 1, j * BLOCK : (j + 1) * BLOCK]
            for i in range(heads // per)
            for j in range(per)
        ]
    else:
        rows = [jnp.concatenate([lines[i : i + 1] for i in range(BLOCK // width)], axis=1)]
    return jnp.concatenate(rows + [jnp.zeros((ROWS - heads, BLOCK), lines.dtype)], axis=0)


def prep_kernel(saved_ref, switch_ref, final_ref, scale_ref, x_ref, dt_ref, out_ref, gate_ref):
    _, _, width = out_ref.shape
    cols = INNER // NORM_GROUPS
    heads = width // HEAD_DIM
    dt_rows = dt_ref[...].astype(f32)
    for n in range(saved_ref.shape[1] // cols):
        at = slice(n * cols, (n + 1) * cols)
        values = saved_ref[:, at].astype(f32)
        switch = switch_ref[:, at].astype(f32)
        cot = final_ref[:, at].astype(f32) * scale_ref[:, at]
        sig = 1.0 / (1.0 + jnp.exp(-switch))
        silu = switch * sig
        g = values * silu
        inv = lax.rsqrt(jnp.mean(g * g, axis=-1, keepdims=True) + EPSILON)
        scaled = g * inv
        d_g = inv * (cot - scaled * jnp.mean(cot * scaled, axis=-1, keepdims=True))
        d_y = (d_g * silu).astype(bf16)
        gate_ref[:, at] = (d_g * values * (sig * (1.0 + switch * (1.0 - sig)))).astype(bf16)
        for c in range(cols // width):
            i = n * (cols // width) + c
            out_ref[i, :BLOCK, :] = x_ref[:, i * width : (i + 1) * width]
            out_ref[i, BLOCK : 2 * BLOCK, :] = d_y[:, c * width : (c + 1) * width]
            out_ref[i, 2 * BLOCK :, :] = pack_rows(
                dt_rows[i * heads : (i + 1) * heads], width
            ).astype(bf16)


def proj_kernel(at_ref, act_ref, *refs):
    count = len(refs) - 2
    own_ref, other_ref = refs[count:]
    size = act_ref.shape[1] // count
    total = jnp.zeros((act_ref.shape[0], refs[0].shape[1]), f32)
    for k in range(count):
        start = pl.multiple_of((at_ref[0] ^ k) * size, size)
        total = total + nn(act_ref[:, pl.ds(start, size)], refs[k][...])
    wide = total.shape[1] // GROUPS
    low = total[:, :wide].astype(bf16)
    high = total[:, wide:].astype(bf16)
    is_low = jnp.broadcast_to(at_ref[2], low.shape) == 0
    own_ref[...] = jnp.where(is_low, low, high)
    other_ref[...] = jnp.where(is_low, high, low)


def hidden_kernel(at_ref, own_ref, other_ref, *refs):
    count = len(refs) - 1
    out_ref = refs[count]
    size = out_ref.shape[1] // count
    own = own_ref[...]
    other = other_ref[...]
    is_low = jnp.broadcast_to(at_ref[2], own.shape) == 0
    both = jnp.concatenate(
        [jnp.where(is_low, own, other), jnp.where(is_low, other, own)], axis=1
    )
    for k in range(count):
        start = pl.multiple_of((at_ref[0] ^ k) * size, size)
        out_ref[:, pl.ds(start, size)] = nt(both, refs[k][...]).astype(bf16)


def weight_kernel(dp, at_ref, *refs):
    grad_refs = refs[:dp]
    act_refs = refs[dp : 2 * dp]
    far_ref, last_ref = refs[2 * dp : 2 * dp + 2]
    out_refs = refs[2 * dp + 2 : -1]
    total_ref = refs[-1]
    total = None
    for k in range(dp):
        for part in range(2):
            far = last_ref[...] if k == dp - 1 else far_ref[k]
            acts = act_refs[k][...] if part == 0 else far
            term = tn(acts, grad_refs[k][part])
            total = term if total is None else total + term
    total_ref[...] = total
    size = out_refs[0].shape[0]
    for k, out_ref in enumerate(out_refs):
        start = pl.multiple_of((at_ref[3] ^ k) * size, size)
        out_ref[...] = total_ref[pl.ds(start, size), :].astype(bf16)


def spread_kernel(half, at_ref, *refs):
    outs = refs[2 * half :]
    size = refs[0].shape[0]
    for part in range(2):
        group = at_ref[2] if part == 0 else 1 - at_ref[2]
        lanes = pl.ds(pl.multiple_of(group * STATE, STATE), STATE)
        for k in range(half):
            rows = pl.ds(pl.multiple_of((at_ref[3] ^ k) * size, size), size)
            chunk = refs[part * half + k][...].astype(f32)
            outs[0][rows, lanes] = chunk[:, :STATE]
            outs[1][rows, lanes] = chunk[:, STATE:]


def gather_kernel(at_ref, drop_ref, *refs):
    for k, ref in enumerate(refs[:-2]):
        refs[-2][k] = ref[...]
    refs[-1][...] = drop_ref[...]


def unpack_kernel(back_ref, dx_ref, dt_ref):
    devices, _, width = back_ref.shape
    heads = width // HEAD_DIM
    rows = []
    for i in range(devices):
        dx_ref[:, i * width : (i + 1) * width] = back_ref[i, :BLOCK, :]
        rows.append(unpack_rows(back_ref[i, BLOCK:, :].astype(f32), heads, width)[:heads])
    dt_ref[...] = jnp.concatenate(rows, axis=0).astype(bf16)


def split(value, count):
    terms = []
    for _ in range(count):
        terms.append(value.astype(bf16))
        value = value - terms[-1].astype(f32)
    return terms


def per_head(ref, line, index):
    total = jnp.zeros(index.shape, f32)
    for h in range(ref.shape[1]):
        total = jnp.where(index == h, ref[line, h], total)
    return total


def triangle(include):
    r = lax.broadcasted_iota(jnp.int32, (BLOCK, BLOCK), 0)
    c = lax.broadcasted_iota(jnp.int32, (BLOCK, BLOCK), 1)
    return jnp.where(include(r, c), 1.0, 0.0).astype(bf16)


def expand(count, width):
    shape = (count * ROWS, width)
    r = lax.broadcasted_iota(jnp.int32, shape, 0) % ROWS
    c = lax.broadcasted_iota(jnp.int32, shape, 1) // HEAD_DIM
    return jnp.where(r == c, 1.0, 0.0)


PAD = 8


def conv(pad_ref, b, w_ref, flip):
    win = pad_ref[pl.ds(pl.multiple_of(b * BLOCK, BLOCK), BLOCK + 2 * PAD), :]
    total = None
    for k in range(CONV_K):
        shift = (CONV_K - 1) // 2 - k
        moved = win if shift == 0 else pltpu.roll(win, shift % (BLOCK + 2 * PAD), 0)
        tap = w_ref[CONV_K - 1 - k : CONV_K - k, :] if flip else w_ref[k : k + 1, :]
        term = moved[PAD : PAD + BLOCK] * tap
        total = term if total is None else total + term
    return total


def enter_kernel(
    head_ref,
    x_ref,
    drop_ref,
    xw_ref,
    u_ref,
    us_ref,
    row_ref,
    wide_ref,
    dr_ref,
    gg_ref,
    xpad,
):
    blocks, _, width = x_ref.shape
    heads = width // HEAD_DIM
    all_rows = blocks * ROWS
    rows_of = lax.broadcasted_iota(jnp.int32, (ROWS, BLOCK), 0)
    offset = per_head(head_ref, 0, rows_of)
    fade = jnp.exp(per_head(head_ref, 1, rows_of))
    xpad[0:PAD, :] = jnp.zeros((PAD, width), f32)
    xpad[PAD + blocks * BLOCK :, :] = jnp.zeros((PAD, width), f32)

    def load_block(b, _):
        at = pl.multiple_of(b * BLOCK, BLOCK) + PAD
        xpad[pl.ds(at, BLOCK), :] = x_ref[b, :BLOCK, :].astype(f32)
        lines = x_ref[b, 2 * BLOCK :, :].astype(f32)
        row_ref[0, b] = unpack_rows(lines, heads, width) + offset
        drop = drop_ref[:, pl.ds(pl.multiple_of(b * BLOCK, BLOCK), BLOCK)]
        row_ref[1, b] = jnp.concatenate([drop, jnp.zeros((ROWS - heads, BLOCK), f32)], axis=0)
        return 0

    lax.fori_loop(0, blocks, load_block, 0)
    raw = row_ref[0].reshape(all_rows, BLOCK)
    dt = jnp.maximum(raw, 0.0) + jnp.log1p(jnp.exp(-jnp.abs(raw)))
    rate = (dt.reshape(blocks, ROWS, BLOCK) * fade[None] + row_ref[1]).reshape(all_rows, BLOCK)
    sums = nn(jnp.concatenate(split(rate, 3), axis=0), triangle(lambda r, c: r <= c))
    cum = sums[:all_rows] + sums[all_rows : 2 * all_rows] + sums[2 * all_rows :]
    total = cum[:, BLOCK - 1 :]
    row_ref[0] = dt.reshape(blocks, ROWS, BLOCK)
    row_ref[1] = cum.reshape(blocks, ROWS, BLOCK)
    row_ref[2] = jnp.exp(-cum).reshape(blocks, ROWS, BLOCK)
    row_ref[3] = jnp.exp(cum - total).reshape(blocks, ROWS, BLOCK)
    row_ref[4] = (1.0 / (1.0 + jnp.exp(-raw))).reshape(blocks, ROWS, BLOCK)

    def body(b, _):
        pre = conv(xpad, b, xw_ref, False)
        sig = 1.0 / (1.0 + jnp.exp(-pre))
        u = pre * sig
        u_ref[b] = u
        us_ref[b] = sig * (1.0 + pre * (1.0 - sig))
        rows = jnp.concatenate([row_ref[0, b], row_ref[2, b], row_ref[3, b]], axis=1)
        wide = tn(jnp.concatenate(split(rows, 3), axis=0), expand(3, width).astype(bf16))
        wide_ref[b] = wide
        w_in = wide[BLOCK : 2 * BLOCK]
        w_out = wide[2 * BLOCK :]
        driven = u * wide[:BLOCK]
        g = x_ref[b, BLOCK : 2 * BLOCK, :].astype(f32)
        dr_ref[b] = jnp.concatenate([driven * w_out, driven * w_in], axis=1).astype(bf16)
        gg_ref[b] = jnp.concatenate([g * w_in, g * w_out], axis=1).astype(bf16)
        return 0

    lax.fori_loop(0, blocks, body, 0, unroll=2)


def mixer_kernel(
    devices,
    at_ref,
    head_ref,
    *refs,
):
    x_ref, u_s, us_s, rows_in, wide_s, dr_s, gg_s, xw_ref, write_ref, read_ref = refs[:10]
    bc_refs = refs[10 : 10 + devices]
    refs = refs[10 + devices :]
    out_ref = refs[0]
    dbc_refs = refs[1 : 1 + devices // 2]
    xpad, bcpad, kcs_s, kr_s, row_s, st_s, car_s, sel_s, bcw_ref, stage, sems = refs[
        1 + devices // 2 :
    ]
    copies = [
        pltpu.make_async_copy(bc_ref, stage.at[k], sems.at[k]) for k, bc_ref in enumerate(bc_refs)
    ]
    for copy in copies:
        copy.start()
    blocks, _, width = x_ref.shape
    heads = width // HEAD_DIM
    pad = PAD
    lanes = min(width, BLOCK)
    per = lanes // HEAD_DIM
    all_rows = blocks * ROWS
    fade = jnp.exp(per_head(head_ref, 1, lax.broadcasted_iota(jnp.int32, (ROWS, BLOCK), 0)))

    mine = pl.ds(pl.multiple_of(at_ref[2] * STATE, STATE), STATE)
    bcw_ref[:CONV_K, :STATE] = write_ref[:, mine]
    bcw_ref[:CONV_K, STATE:] = read_ref[:, mine]

    r = lax.broadcasted_iota(jnp.int32, (5 * width, BLOCK), 0)
    c = lax.broadcasted_iota(jnp.int32, (5 * width, BLOCK), 1)
    base = jnp.where(r < 2 * width, 0, jnp.where(r < 4 * width, ROWS, 2 * ROWS))
    sel_s[...] = jnp.where(c == base + (r % width) // HEAD_DIM, 1.0, 0.0).astype(bf16)

    xpad[0:pad, :] = jnp.zeros((pad, width), f32)
    xpad[pad + blocks * BLOCK :, :] = jnp.zeros((pad, width), f32)
    bcpad[0:pad, :] = jnp.zeros((pad, 2 * STATE), f32)
    bcpad[pad + blocks * BLOCK :, :] = jnp.zeros((pad, 2 * STATE), f32)
    for k, copy in enumerate(copies):
        copy.wait()
        at = pl.multiple_of((at_ref[1] ^ k) * BLOCK, BLOCK) + pad
        bcpad[pl.ds(at, BLOCK), :] = stage[k].astype(f32)

    def first(b, _):
        pre = conv(bcpad, b, bcw_ref, False)
        sig = 1.0 / (1.0 + jnp.exp(-pre))
        act = (pre * sig).astype(bf16)
        kcs_s[b] = sig * (1.0 + pre * (1.0 - sig))
        kr_s[b] = act
        st_s[b, :, : 2 * width] = tn(act[:, :STATE], dr_s[b])
        st_s[b, :, 2 * width :] = tn(act[:, STATE:], gg_s[b])
        return 0

    lax.fori_loop(0, blocks, first, 0, unroll=2)

    def scan(slot, back):
        def step(i, carry):
            b = blocks - 1 - i if back else i
            at = slice(slot * width, (slot + 1) * width)
            car_s[b, :, at] = carry.astype(bf16)
            decay = wide_s[b][2 * BLOCK - 1 : 2 * BLOCK]
            return carry * decay + st_s[b, :, at]

        lax.fori_loop(0, blocks, step, jnp.zeros((STATE, width), f32), unroll=4)

    scan(0, False)
    scan(1, True)
    scan(2, True)
    scan(3, False)

    def second(b, _):
        act = kr_s[b]
        keys = act[:, :STATE]
        reads = act[:, STATE:]
        u = u_s[b]
        g16 = x_ref[b, BLOCK : 2 * BLOCK, :]
        cum = rows_in[1, b]
        cum_t = cum.T
        wide = wide_s[b]
        w_dt = wide[:BLOCK]
        w_in = wide[BLOCK : 2 * BLOCK]
        w_out = wide[2 * BLOCK :]
        driven = (u * w_dt).astype(bf16)
        d_io = dr_s[b]
        g_io = gg_s[b]
        carry = car_s[b]
        c_s = carry[:, : 2 * width]
        c_g = carry[:, 2 * width :]
        y = nn(reads, c_s)
        c = nn(keys, c_g)
        d_r = nt(g_io, c_s)
        d_k = nt(d_io, c_g)
        scores = nt(keys, reads)
        upper = lax.broadcasted_iota(jnp.int32, (BLOCK, BLOCK), 0) > lax.broadcasted_iota(
            jnp.int32, (BLOCK, BLOCK), 1
        )
        lane = lax.broadcasted_iota(jnp.int32, (BLOCK, lanes), 1) // HEAD_DIM
        column = lax.broadcasted_iota(jnp.int32, (BLOCK, BLOCK), 1)
        row = lax.broadcasted_iota(jnp.int32, (ROWS, BLOCK), 0)
        d_scores = None
        d_driven = []
        by_key = jnp.zeros((BLOCK, BLOCK), f32)
        by_read = jnp.zeros((ROWS, BLOCK), f32)
        none = jnp.zeros((BLOCK, lanes), bf16)
        for p in range(width // lanes):
            at = slice(p * lanes, (p + 1) * lanes)
            g_p = g16[:, at]
            d_p = driven[:, at]
            gu = nt(
                jnp.concatenate([jnp.where(lane == j, d_p, none) for j in range(per)], axis=0), g_p
            )
            s_p = []
            for j in range(per):
                h = p * per + j
                decay = jnp.exp(-jnp.abs(cum_t[:, h : h + 1] - cum[h : h + 1, :]))
                gu_h = gu[j * BLOCK : (j + 1) * BLOCK]
                s = scores * decay
                term = gu_h * decay
                d_scores = term if d_scores is None else d_scores + term
                z = s * gu_h
                z = jnp.where(upper, z, -z)
                by_key = jnp.where(column == h, jnp.sum(z, axis=1, keepdims=True), by_key)
                by_read = jnp.where(row == h, jnp.sum(z, axis=0, keepdims=True), by_read)
                s_p.append(s.astype(bf16))
            d_driven.append(
                nn(
                    jnp.concatenate(s_p, axis=1),
                    jnp.concatenate([jnp.where(lane == j, g_p, none) for j in range(per)], axis=0),
                )
            )
        ds16 = d_scores.astype(bf16)
        d_k = d_k + nn(ds16, reads)
        d_r = d_r + tn(ds16, keys)
        c_x = c[:, :width]
        c_y = c[:, width:]
        d_dr = jnp.concatenate(d_driven, axis=1) + w_out * c_x + w_in * c_y
        prefix = d_io[:, :width].astype(f32) * c_x + g_io[:, width:].astype(f32) * y[:, width:]
        suffix = g_io[:, :width].astype(f32) * y[:, :width] + d_io[:, width:].astype(f32) * c_y
        sums = nn(
            jnp.concatenate(
                split(suffix - prefix, 2) + split(prefix, 2) + [(d_dr * u).astype(bf16)], axis=1
            ),
            sel_s[...],
        )
        sums = sums.T
        by_key = by_key.T
        through = jnp.sum(c_s.astype(f32) * c_g.astype(f32), axis=0, keepdims=True)
        through = (through[:, :width] + through[:, width:]) * wide[2 * BLOCK - 1 : 2 * BLOCK]
        through = jnp.sum(expand(1, width) * through, axis=1, keepdims=True)
        before = jnp.sum(sums[ROWS : 2 * ROWS], axis=1, keepdims=True) + through
        row_s[0, b] = sums[:ROWS] + by_key[:ROWS] - by_read
        row_s[1, b] = jnp.broadcast_to(before, (ROWS, BLOCK))
        row_s[2, b] = sums[2 * ROWS : 3 * ROWS]
        skip = per_head(head_ref, 2, lax.broadcasted_iota(jnp.int32, (1, width), 1) // HEAD_DIM)
        d_u = d_dr * w_dt + g16.astype(f32) * skip
        at = pl.multiple_of(b * BLOCK, BLOCK) + pad
        xpad[pl.ds(at, BLOCK), :] = d_u * us_s[b]
        bcpad[pl.ds(at, BLOCK), :] = jnp.concatenate([d_k, d_r], axis=1) * kcs_s[b]
        return 0

    lax.fori_loop(0, blocks, second, 0, unroll=4)

    sums = nn(
        jnp.concatenate(split(row_s[0].reshape(all_rows, BLOCK), 3), axis=0),
        triangle(lambda r, c: r >= c),
    )
    sums = sums[:all_rows] + sums[all_rows : 2 * all_rows] + sums[2 * all_rows :]
    d_rate = -(sums.reshape(blocks, ROWS, BLOCK) + row_s[1])
    row_s[0] = (row_s[2] + d_rate * fade[None]) * rows_in[4]

    for k, dbc_ref in enumerate(dbc_refs):
        for part in range(2):
            b = at_ref[1] ^ k if part == 0 else at_ref[1] ^ k ^ len(dbc_refs)
            dbc_ref[part] = conv(bcpad, b, bcw_ref, True).astype(bf16)

    def last(b, _):
        out_ref[b, :BLOCK, :] = conv(xpad, b, xw_ref, True).astype(bf16)
        out_ref[b, BLOCK:, :] = pack_rows(row_s[0, b][:heads], width).astype(bf16)
        return 0

    lax.fori_loop(0, blocks, last, 0, unroll=2)


def limit(mib):
    return pltpu.CompilerParams(vmem_limit_bytes=mib << 20)


def vmem():
    return pl.BlockSpec(memory_space=pltpu.VMEM)


def smem():
    return pl.BlockSpec(memory_space=pltpu.SMEM)


def run_enter(per_heads, x, drop, xw):
    blocks, _, width = x.shape
    shape = jax.ShapeDtypeStruct
    return pl.pallas_call(
        enter_kernel,
        out_shape=(
            shape((blocks, BLOCK, width), f32),
            shape((blocks, BLOCK, width), f32),
            shape((5, blocks, ROWS, BLOCK), f32),
            shape((blocks, 3 * BLOCK, width), f32),
            shape((blocks, BLOCK, 2 * width), bf16),
            shape((blocks, BLOCK, 2 * width), bf16),
        ),
        in_specs=[smem()] + [vmem()] * 3,
        out_specs=(vmem(),) * 6,
        scratch_shapes=[pltpu.VMEM((blocks * BLOCK + 2 * PAD, width), f32)],
        compiler_params=limit(min(60, 24 * max(1, blocks // 8))),
        name="enter",
    )(per_heads, x, drop, xw)


def run_mixer(at, per_heads, x, entered, filters, bc):
    blocks, _, width = x.shape
    length = blocks * BLOCK
    scratch = [
        pltpu.VMEM((length + 2 * PAD, width), f32),
        pltpu.VMEM((length + 2 * PAD, 2 * STATE), f32),
        pltpu.VMEM((blocks, BLOCK, 2 * STATE), f32),
        pltpu.VMEM((blocks, BLOCK, 2 * STATE), bf16),
        pltpu.VMEM((3, blocks, ROWS, BLOCK), f32),
        pltpu.VMEM((blocks, STATE, 4 * width), f32),
        pltpu.VMEM((blocks, STATE, 4 * width), bf16),
        pltpu.VMEM((5 * width, BLOCK), bf16),
        pltpu.VMEM((ROWS, 2 * STATE), f32),
        pltpu.VMEM((len(bc), BLOCK, 2 * STATE), bf16),
        pltpu.SemaphoreType.DMA((len(bc),)),
    ]
    half = len(bc) // 2
    outs = pl.pallas_call(
        functools.partial(mixer_kernel, len(bc)),
        out_shape=(jax.ShapeDtypeStruct((blocks, BLOCK + EXTRA, width), bf16),)
        + (jax.ShapeDtypeStruct((2, BLOCK, 2 * STATE), bf16),) * half,
        in_specs=[smem()] * 2
        + [vmem()] * 10
        + [pl.BlockSpec(memory_space=pltpu.HBM)] * len(bc),
        out_specs=(vmem(),) * (1 + half),
        scratch_shapes=scratch,
        compiler_params=limit(min(60, 40 * max(1, blocks // 8))),
        name="mixer",
    )(at, per_heads, x, *entered, *filters, *bc)
    return outs[0], outs[1:]


def swap(value, axis, bits):
    size = lax.axis_size(axis)
    return lax.ppermute(value, axis, [(i, i ^ bits) for i in range(size)])


def call(kernel, outs, *args, scratch=()):
    specs = [smem()] + [vmem()] * (len(args) - 1)
    return pl.pallas_call(
        kernel,
        out_shape=outs,
        in_specs=specs,
        out_specs=jax.tree.map(lambda _: vmem(), outs),
        scratch_shapes=scratch,
        compiler_params=limit(16),
    )(*args)


def local(
    layer_activity,
    writer_matrix,
    reader_matrix,
    source_unfiltered,
    switch_raw_signal,
    saved_result,
    final_adjoint,
    delta_raw,
    extra_logdrop,
    source_filter_coefs,
    writer_filter_coefs,
    reader_filter_coefs,
    delta_offset,
    fading_exponents,
    direct_factor,
    rescale_factor,
):
    tokens = layer_activity.shape[1]
    width_in = layer_activity.shape[2]
    dp = lax.axis_size("dp")
    sp = lax.axis_size("sp")
    half = sp // 2
    heads = delta_offset.shape[0]
    width = heads * HEAD_DIM
    me_d = lax.axis_index("dp")
    me_s = lax.axis_index("sp")
    at = jnp.stack([me_d, me_s, me_s // half, me_s % half]).astype(jnp.int32)
    shape = jax.ShapeDtypeStruct
    rows = layer_activity[0]
    share = width_in // dp

    weights = jnp.concatenate(
        [
            m[:, g * STATE : (g + 1) * STATE]
            for g in range(GROUPS)
            for m in (writer_matrix, reader_matrix)
        ],
        axis=1,
    )
    pieces = {0: weights}
    bit = dp // 2
    while bit:
        moved = {k ^ bit: swap(v, "dp", bit) for k, v in list(pieces.items())}
        pieces.update(moved)
        bit //= 2
    pieces = [pieces[k] for k in range(dp)]

    steps = NORM_GROUPS // 2
    wide = INNER // steps
    row_spec = pl.BlockSpec((tokens, wide), lambda i: (0, i))
    packed, d_gate = pl.pallas_call(
        prep_kernel,
        grid=(steps,),
        in_specs=[
            row_spec,
            row_spec,
            row_spec,
            pl.BlockSpec((1, wide), lambda i: (0, i)),
            row_spec,
            pl.BlockSpec((HEADS // steps, tokens), lambda i: (i, 0)),
        ],
        out_specs=(
            pl.BlockSpec((sp // steps, 2 * BLOCK + EXTRA, width), lambda i: (i, 0, 0)),
            row_spec,
        ),
        out_shape=(
            shape((sp, 2 * BLOCK + EXTRA, width), bf16),
            shape((tokens, INNER), bf16),
        ),
        name="prep",
    )(
        saved_result[0],
        switch_raw_signal[0],
        final_adjoint[0],
        rescale_factor[None],
        source_unfiltered[0],
        delta_raw[0].T,
    )
    heads_x = lax.all_to_all(packed, "sp", 0, 0, tiled=True)

    acts = [lax.dynamic_slice(rows, (0, (me_d ^ k) * share), (tokens, share)) for k in range(dp)]
    acts = [acts[0]] + [swap(acts[k], "dp", k) for k in range(1, dp)]
    drop = extra_logdrop[0].T
    gathered, drop = call(
        gather_kernel,
        (shape((dp - 1, tokens, share), bf16), shape(drop.shape, f32)),
        at,
        drop,
        *acts[: dp - 1],
    )
    acts += [swap(gathered, "sp", half), swap(acts[dp - 1], "sp", half)]

    bc = shape((tokens, 2 * STATE), bf16)
    own, other = call(proj_kernel, (bc, bc), at, rows, *pieces)
    other = swap(other, "sp", half)
    all_bc = [own if k == 0 else swap(own, "sp", k) for k in range(half)]
    all_bc += [other if k == 0 else swap(other, "sp", k) for k in range(half)]

    per_heads = jnp.stack([delta_offset, fading_exponents, direct_factor])
    entered = run_enter(per_heads, heads_x, drop, source_filter_coefs)
    filters = (source_filter_coefs, writer_filter_coefs, reader_filter_coefs)
    d_x, d_bc = run_mixer(at, per_heads, heads_x, entered, filters, all_bc)

    parts = [d_bc[0]] + [swap(d_bc[k], "sp", k) for k in range(1, half)]
    grads = functools.reduce(jnp.add, [p.astype(f32) for p in parts]).astype(bf16)
    back_x = lax.all_to_all(d_x, "sp", 0, 0, tiled=True)
    all_grads = [grads if k == 0 else swap(grads, "dp", k) for k in range(dp)]
    rest = swap(grads[1], "sp", half)

    chunk = shape((share // half, 2 * STATE), bf16)
    chunks = call(
        functools.partial(weight_kernel, dp),
        (chunk,) * half,
        at,
        *all_grads,
        *acts,
        scratch=[pltpu.VMEM((share, 2 * STATE), f32)],
    )
    chunks = [chunks[0]] + [swap(chunks[k], "sp", k) for k in range(1, half)]
    mine = functools.reduce(jnp.add, [c.astype(f32) for c in chunks]).astype(bf16)
    theirs = swap(mine, "sp", half)
    placed = [mine if k == 0 else swap(mine, "sp", k) for k in range(half)]
    placed += [theirs if k == 0 else swap(theirs, "sp", k) for k in range(half)]

    d_hidden = call(hidden_kernel, shape((tokens, width_in), bf16), at, grads[0], rest, *pieces)
    d_source, d_delta = pl.pallas_call(
        unpack_kernel,
        out_shape=(shape((tokens, INNER), bf16), shape((HEADS, tokens), bf16)),
        in_specs=[vmem()],
        out_specs=(vmem(), vmem()),
        compiler_params=limit(16),
        name="unpack",
    )(back_x)
    matrix = shape((share, GROUPS * STATE), f32)
    d_w_b, d_w_c = call(functools.partial(spread_kernel, half), (matrix, matrix), at, *placed)
    return d_hidden[None], d_source[None], d_gate[None], d_delta.T[None], d_w_b, d_w_c


def solution(mesh):
    in_specs = (
        P("dp", "sp", None),
        P("dp", None),
        P("dp", None),
        P("dp", "sp", None),
        P("dp", "sp", None),
        P("dp", "sp", None),
        P("dp", "sp", None),
        P("dp", "sp", None),
        P("dp", None, "sp"),
        P(None, "sp"),
        P(),
        P(),
        P("sp"),
        P("sp"),
        P("sp"),
        P(),
    )
    out_specs = (
        P("dp", "sp", None),
        P("dp", "sp", None),
        P("dp", "sp", None),
        P("dp", "sp", None),
        P("dp", None),
        P("dp", None),
    )

    return jax.shard_map(local, mesh=mesh, in_specs=in_specs, out_specs=out_specs, check_vma=False)
```
